32 devices in a mesh: grp: 2 (over y), kv: 4 (over z), tp: 4 (over x, core).
Axes of the slice: x: 2, y: 2, z: 4, core: 2. Of those that a mesh axis runs over, the one named last changes fastest.
Arguments:
- stream: bfloat16 [256, 2048], P('grp', ('kv', 'tp')), parts along dimension 0, may hold values from -72 to 72
- lengths: int32 [256], P(('grp', 'kv')), parts along dimension 0, may hold values from 1 to 8, 384 in all
- delta_state: float32 [256, 32, 128, 128], P(('grp', 'kv'), 'tp'), parts along dimension 0, may hold values from -0.6 to 0.6
- q_hist: bfloat16 [256, 3, 2048], P(('grp', 'kv'), None, 'tp'), parts along dimension 0, may hold values from -6 to 6
- k_hist: bfloat16 [256, 3, 2048], P(('grp', 'kv'), None, 'tp'), parts along dimension 0, may hold values from -6 to 6
- v_hist: bfloat16 [256, 3, 4096], P(('grp', 'kv'), None, 'tp'), parts along dimension 0, may hold values from -6 to 6
- norm_gain: bfloat16 [2048], replicated, may hold values from 0.099609375 to 1.8984375
- w_query: bfloat16 [2048, 2048], P('kv', 'tp'), may hold values from -0.125 to 0.125
- w_key: bfloat16 [2048, 2048], P('kv', 'tp'), may hold values from -0.125 to 0.125
- w_value: bfloat16 [2048, 4096], P('kv', 'tp'), may hold values from -0.125 to 0.125
- w_gate: bfloat16 [2048, 4096], P('kv', 'tp'), may hold values from -0.125 to 0.125
- w_beta: bfloat16 [2048, 32], replicated, may hold values from -0.125 to 0.125
- w_decay: bfloat16 [2048, 32], replicated, may hold values from -0.125 to 0.125
- conv_query: bfloat16 [4, 2048], replicated, may hold values from -3 to 3
- conv_key: bfloat16 [4, 2048], replicated, may hold values from -3 to 3
- conv_value: bfloat16 [4, 4096], replicated, may hold values from -3 to 3
- decay_log: float32 [32], replicated, may hold values from 0 to 2.77
- time_bias: float32 [32], replicated, may hold values from -4 to 0
- out_gain: bfloat16 [128], replicated, may hold values from 0.099609375 to 1.8984375
- w_out: bfloat16 [4096, 2048], P('tp', 'kv'), may hold values from -0.09375 to 0.09375
- mlp_gain: bfloat16 [2048], replicated, may hold values from 0.099609375 to 1.8984375
- w_up: bfloat16 [2048, 8192], P('kv', 'tp'), may hold values from -0.125 to 0.125
- w_down: bfloat16 [8192, 2048], P('tp', 'kv'), may hold values from -0.0625 to 0.0625
Outputs:
- result: bfloat16 [256, 2048], P('grp', ('kv', 'tp')), parts along dimension 0
- new_state: float32 [256, 32, 128, 128], P(('grp', 'kv'), 'tp'), parts along dimension 0
The draws below stay inside these ranges and needn't reach their ends.
There are 2 independent parts, one for each index of `grp`. The reference program is written for one: setup_inputs(seed, part) draws one part's arguments, and reference() takes and returns one part's arrays. A program takes and returns all parts, laid end to end along the dimension named above; an argument that names none is the same for every part. Nothing has to cross between parts.
All inputs are finite; a program needn't handle non-finite values. No bound on the sum of `lengths` on one device may be relied on, other than what follows from the above.
Results may differ from the reference program's by a relative error of at most 0.01.
Values may be sent and summed in bfloat16 or wider, within the bound.
No kernel may reach another device: no remote copies, remote signals or barrier semaphores. Data moves between devices by JAX's collectives and lax.ppermute only.
A program may use at most 128 MiB of HBM per device.

```python
import math
import jax
import jax.numpy as jnp
import numpy as np
from jax import lax

D = 2048
HEADS_K = 16
HEADS_V = 32
HEAD_DIM = 128
FF_UNITS = 8192
CONV = 4
SEQS = 128
N_KV = 4
N_TP = 4


def draw_stream(key, part):
    first_key, second_key, third_key = jax.random.split(jax.random.fold_in(key, 11), 3)
    columns = jnp.arange(D)
    block_number = columns // (D // N_KV)
    piece_number = columns // (D // (N_KV * N_TP)) % N_TP
    rising = 3.0 ** (block_number / max(N_KV - 1, 1)) * 3.0 ** (piece_number / max(N_TP - 1, 1))
    roughness = jax.random.uniform(first_key, (D,), jnp.float32, 0.5, 1.5)
    row_factor = jnp.exp(jax.random.uniform(second_key, (SEQS, 1), jnp.float32, 0.0, math.log(4.0)))
    base_values = jnp.clip(jax.random.normal(third_key, (SEQS, D), jnp.float32), -4.0, 4.0)
    return (base_values * rising * roughness * row_factor / 3.0).astype(jnp.bfloat16)


def block_scale(own_key, extent, cuts, smallest, largest):
    def one(dim, parts):
        steps = jax.random.uniform(jax.random.fold_in(jax.random.fold_in(own_key, 6), dim), (parts,), jnp.float32, smallest / len(cuts), largest / len(cuts))
        return jnp.repeat(jnp.exp(steps), extent[dim] // parts).reshape((-1,) + (1,) * (len(extent) - dim - 1))

    loudness = one(*cuts[0])
    for cut in cuts[1:]:
        loudness = loudness * one(*cut)
    return loudness


def profile(amount, total, reach, skew):
    portions = [(1 << 20) // math.isqrt(standing ** skew) + 1 for standing in range(2, amount + 1)]
    surplus, holding = total - reach - (amount - 1), [1] * (amount - 1)
    while surplus > 0:
        movable = [i for i in range(amount - 1) if holding[i] < reach]
        whole, remaining = sum([portions[i] for i in movable]), surplus
        for i in movable:
            extra = min(reach - holding[i], max(1, remaining * portions[i] // whole), surplus)
            holding[i] = holding[i] + extra
            surplus = surplus - extra
    return np.array([reach] + holding)


def uneven(rng, count, total, most, skew):
    if count == 2:
        one = jax.random.randint(rng, (), max(1, total - most), min(most, total - 1) + 1)
        return jnp.stack([one, total - one])
    sizes = jnp.asarray(profile(count, total, most, skew), jnp.int32)
    pairs = (count - 1) // 2
    donor, taker = sizes[1:1 + 2 * pairs:2], sizes[2:2 + 2 * pairs:2]
    room = jnp.minimum(donor - 1, most - taker)
    passed = jax.random.randint(jax.random.fold_in(rng, 1), (pairs,), 0, 1 << 20) % (room + 1)
    sizes = sizes.at[1:1 + 2 * pairs:2].set(donor - passed).at[2:2 + 2 * pairs:2].set(taker + passed)
    return sizes[jax.random.permutation(jax.random.fold_in(rng, 2), count)]


def normal_values(rng, extent, scale, most, cuts=(), held_as=jnp.bfloat16):
    drawn = scale * jax.random.normal(rng, extent, jnp.float32)
    if cuts:
        drawn = drawn * block_scale(rng, extent, cuts, -0.22, 0.18)
    return jnp.clip(drawn, -most, most).astype(held_as)


def setup_inputs(seed: int = 0, part: int = 0) -> dict:
    key_list = jax.random.split(jax.random.key(seed), 24)
    own_keys = jax.random.split(jax.random.fold_in(key_list[23], part), 24)
    stream = draw_stream(jax.random.fold_in(jax.random.fold_in(key_list[23], part), 71), part)
    lengths = uneven(own_keys[1], SEQS, 3 * SEQS, 8, 2).astype(jnp.int32)
    delta_state = normal_values(own_keys[2], (SEQS, HEADS_V, HEAD_DIM, HEAD_DIM), 0.1, 0.6, ((0, 4), (1, 4)), jnp.float32)
    q_hist = normal_values(own_keys[3], (SEQS, CONV - 1, HEADS_K * HEAD_DIM), 1.0, 6.0, ((0, 4), (2, 4)))
    k_hist = normal_values(own_keys[4], (SEQS, CONV - 1, HEADS_K * HEAD_DIM), 1.0, 6.0, ((0, 4), (2, 4)))
    v_hist = normal_values(own_keys[5], (SEQS, CONV - 1, HEADS_V * HEAD_DIM), 1.0, 6.0, ((0, 4), (2, 4)))
    norm_gain = jnp.clip(1.0 + 0.18 * jax.random.normal(key_list[6], (D,), jnp.float32), 0.099609375, 1.8984375).astype(jnp.bfloat16)
    w_query = normal_values(key_list[7], (D, HEADS_K * HEAD_DIM), D ** -0.5, 0.125, ((0, 4), (1, 4)))
    w_key = normal_values(key_list[8], (D, HEADS_K * HEAD_DIM), D ** -0.5, 0.125, ((0, 4), (1, 4)))
    w_value = normal_values(key_list[9], (D, HEADS_V * HEAD_DIM), D ** -0.5, 0.125, ((0, 4), (1, 4)))
    w_gate = normal_values(key_list[10], (D, HEADS_V * HEAD_DIM), D ** -0.5, 0.125, ((0, 4), (1, 4)))
    w_beta = normal_values(key_list[11], (D, HEADS_V), D ** -0.5, 0.125)
    w_decay = normal_values(key_list[12], (D, HEADS_V), D ** -0.5, 0.125)
    conv_query = normal_values(key_list[13], (CONV, HEADS_K * HEAD_DIM), CONV ** -0.5, 3.0)
    conv_key = normal_values(key_list[14], (CONV, HEADS_K * HEAD_DIM), CONV ** -0.5, 3.0)
    conv_value = normal_values(key_list[15], (CONV, HEADS_V * HEAD_DIM), CONV ** -0.5, 3.0)
    decay_log = jnp.clip(jax.random.uniform(key_list[16], (HEADS_V,), jnp.float32, 0.0, 2.77), 0.0, 2.77)
    time_bias = jnp.clip(jax.random.uniform(key_list[17], (HEADS_V,), jnp.float32, -4.0, 0.0), -4.0, 0.0)
    out_gain = jnp.clip(1.0 + 0.18 * jax.random.normal(key_list[18], (HEAD_DIM,), jnp.float32), 0.099609375, 1.8984375).astype(jnp.bfloat16)
    w_out = normal_values(key_list[19], (HEADS_V * HEAD_DIM, D), (HEADS_V * HEAD_DIM) ** -0.5, 0.09375, ((0, 4), (1, 4)))
    mlp_gain = jnp.clip(1.0 + 0.18 * jax.random.normal(key_list[20], (D,), jnp.float32), 0.099609375, 1.8984375).astype(jnp.bfloat16)
    w_up = normal_values(key_list[21], (D, FF_UNITS), D ** -0.5, 0.125, ((0, 4), (1, 4)))
    w_down = normal_values(key_list[22], (FF_UNITS, D), FF_UNITS ** -0.5, 0.0625, ((0, 4), (1, 4)))
    return {"stream": stream, "lengths": lengths, "delta_state": delta_state, "q_hist": q_hist, "k_hist": k_hist, "v_hist": v_hist, "norm_gain": norm_gain, "w_query": w_query, "w_key": w_key, "w_value": w_value, "w_gate": w_gate, "w_beta": w_beta, "w_decay": w_decay, "conv_query": conv_query, "conv_key": conv_key, "conv_value": conv_value, "decay_log": decay_log, "time_bias": time_bias, "out_gain": out_gain, "w_out": w_out, "mlp_gain": mlp_gain, "w_up": w_up, "w_down": w_down}


EPSILON = 1e-06

def unit_rows(values, factor):
    return values * lax.rsqrt(lax.optimization_barrier(jnp.sum(values * values, axis=-1, keepdims=True)) + EPSILON) * factor

def short_filter(current, history, weights, live_rows):
    history_live = jnp.where(live_rows[:, :, None], history.astype(jnp.float32), 0.0)
    filter_taps = weights.astype(jnp.float32)
    filtered = current * filter_taps[-1] + lax.optimization_barrier(jnp.sum(history_live * filter_taps[None, :-1], axis=1))
    return jax.nn.silu(filtered)

def delta_step(delta_state, fresh_rows, queries, keys_now, values_now, strength, log_fade):
    fade_factor = jnp.exp(log_fade)[:, :, None, None]
    carried = jnp.where(fresh_rows[:, None, None, None], 0.0, delta_state) * fade_factor
    recalled = lax.optimization_barrier(jnp.sum(carried * keys_now[:, :, :, None], axis=2))
    update = strength[:, :, None] * (values_now - recalled)
    new_state = carried + keys_now[:, :, :, None] * update[:, :, None, :]
    readout = lax.optimization_barrier(jnp.sum(new_state * queries[:, :, :, None], axis=2))
    return (new_state, readout)

def gated_norm(readout, gain, gate_in):
    normed = readout * lax.rsqrt(lax.optimization_barrier(jnp.mean(readout * readout, axis=-1, keepdims=True)) + EPSILON)
    return (normed * gain.astype(jnp.float32) * jax.nn.silu(gate_in)).astype(jnp.bfloat16)

def reference(stream, lengths, delta_state, q_hist, k_hist, v_hist, norm_gain, w_query, w_key, w_value, w_gate, w_beta, w_decay, conv_query, conv_key, conv_value, decay_log, time_bias, out_gain, w_out, mlp_gain, w_up, w_down):
    sequences = stream.shape[0]
    stream_wide = stream.astype(jnp.float32)
    row_scale = lax.rsqrt(lax.optimization_barrier(jnp.sum(stream_wide * stream_wide, axis=1, keepdims=True)) / D + EPSILON)
    scaled = (stream_wide * norm_gain.astype(jnp.float32)).astype(jnp.bfloat16)

    def project(weight):
        return jnp.dot(scaled, weight, preferred_element_type=jnp.float32) * row_scale
    live_rows = jnp.arange(CONV - 1, dtype=jnp.int32)[None, :] >= (CONV - lengths)[:, None]
    queries = short_filter(project(w_query), q_hist, conv_query, live_rows)
    keys_now = short_filter(project(w_key), k_hist, conv_key, live_rows)
    values_now = short_filter(project(w_value), v_hist, conv_value, live_rows)
    gate_in = project(w_gate).reshape(sequences, HEADS_V, HEAD_DIM)
    repeat_count = HEADS_V // HEADS_K
    queries = jnp.repeat(unit_rows(queries.reshape(sequences, HEADS_K, HEAD_DIM), HEAD_DIM ** (-0.5)), repeat_count, axis=1)
    keys_now = jnp.repeat(unit_rows(keys_now.reshape(sequences, HEADS_K, HEAD_DIM), 1.0), repeat_count, axis=1)
    values_now = values_now.reshape(sequences, HEADS_V, HEAD_DIM)
    strength = jax.nn.sigmoid(project(w_beta))
    log_fade = -jnp.exp(decay_log) * jax.nn.softplus(project(w_decay) + time_bias)
    new_state, readout = delta_step(delta_state, lengths == 1, queries, keys_now, values_now, strength, log_fade)
    gated = gated_norm(readout, out_gain, gate_in).reshape(sequences, HEADS_V * HEAD_DIM)
    mixed = (stream_wide + jnp.dot(gated, w_out, preferred_element_type=jnp.float32)).astype(jnp.bfloat16)
    mixed_wide = mixed.astype(jnp.float32)
    unit_scale = lax.rsqrt(lax.optimization_barrier(jnp.sum(mixed_wide * mixed_wide, axis=1, keepdims=True)) / D + EPSILON)
    scaled_mix = (mixed_wide * mlp_gain.astype(jnp.float32)).astype(jnp.bfloat16)
    unit_terms = jnp.dot(scaled_mix, w_up, preferred_element_type=jnp.float32) * unit_scale
    hidden = jnp.square(jax.nn.relu(unit_terms)).astype(jnp.bfloat16)
    result = (mixed_wide + jnp.dot(hidden, w_down, preferred_element_type=jnp.float32)).astype(jnp.bfloat16)
    return (result, new_state)
```

```python
import functools

import jax
import jax.numpy as jnp
from jax import lax
from jax.experimental import pallas as pl
from jax.experimental.pallas import tpu as pltpu
from jax.sharding import PartitionSpec as P

EPSILON = 1e-06
LANES = 128
F32 = jnp.float32
BF16 = jnp.bfloat16


def shape_of(shape, dtype):
    return jax.ShapeDtypeStruct(shape, dtype)


def call(body, outs, *args, scratch=(), name):
    return pl.pallas_call(
        body,
        out_shape=outs,
        scratch_shapes=list(scratch),
        name=name,
        compiler_params=pltpu.CompilerParams(vmem_limit_bytes=48 * 1024 * 1024),
    )(*args)


def send(values, axis, distance):
    size = lax.axis_size(axis)
    return lax.ppermute(values, axis, [(i, i ^ distance) for i in range(size)])


def exchange(blocks, axis):
    got = {m: send(blocks[m], axis, m) for m in reversed(range(1, len(blocks)))}
    return [got[m] for m in range(1, len(blocks))]


def silu(values):
    return values * jax.nn.sigmoid(values)


def query_key_kernel(
    place, *refs, pieces, rows_block, n_kv, model_width
):
    piece_refs = refs[:pieces]
    gain_ref, w_query_ref, w_key_ref, w_small_ref = refs[pieces : pieces + 4]
    scaled_ref, own_ref = refs[pieces + 4 : pieces + 6]
    out_refs = refs[pieces + 6 :]
    kv_place, tp_place = place[0], place[1]
    squares = [0.0] * n_kv
    for m in range(pieces):
        width = piece_refs[m].shape[1]
        first = pl.multiple_of((tp_place ^ m) * width, width)
        gain = gain_ref[0:1, pl.ds(first, width)].astype(F32)
        for d in range(n_kv):
            row = pl.multiple_of((kv_place ^ d) * rows_block, rows_block)
            wide = piece_refs[m][pl.ds(row, rows_block), :].astype(F32)
            squares[d] = squares[d] + jnp.sum(wide * wide, axis=1, keepdims=True)
            scaled_ref[d * rows_block : (d + 1) * rows_block, pl.ds(first, width)] = (
                wide * gain
            ).astype(BF16)
    scaled = scaled_ref[...]
    key_cols = w_query_ref.shape[1]
    small_cols = w_small_ref.shape[1]
    for index, w_ref in enumerate((w_query_ref, w_key_ref)):
        part = jnp.dot(scaled, w_ref[...], preferred_element_type=F32)
        first = index * key_cols
        own_ref[:, first : first + key_cols] = part[:rows_block]
        for d in range(1, n_kv):
            out_refs[d - 1][:, first : first + key_cols] = part[
                d * rows_block : (d + 1) * rows_block
            ].astype(BF16)
    small = jnp.dot(scaled, w_small_ref[...], preferred_element_type=F32)
    small = jnp.pad(small, ((0, 0), (0, LANES - small_cols)))
    lane = lax.broadcasted_iota(jnp.int32, (rows_block, LANES), 1)
    half = LANES // 2
    for d in range(n_kv):
        block = small[d * rows_block : (d + 1) * rows_block]
        block = jnp.where(lane == half - 1, squares[d], block)
        if d == 0:
            own_ref[:, 2 * key_cols :] = block
        else:
            high = block.astype(BF16)
            low = (block - high.astype(F32)).astype(BF16)
            out_refs[d - 1][:, 2 * key_cols :] = jnp.where(
                lane < half, high.astype(F32), pltpu.roll(low.astype(F32), half, 1)
            ).astype(BF16)


def value_gate_kernel(scaled_ref, w_value_ref, w_gate_ref, *refs, rows_block, n_kv):
    scaled = scaled_ref[...]
    for index, w_ref in enumerate((w_value_ref, w_gate_ref)):
        own_ref = refs[index]
        out_refs = refs[2 + index * (n_kv - 1) : 2 + (index + 1) * (n_kv - 1)]
        part = jnp.dot(scaled, w_ref[...], preferred_element_type=F32)
        own_ref[...] = part[:rows_block]
        for d in range(1, n_kv):
            out_refs[d - 1][...] = part[d * rows_block : (d + 1) * rows_block].astype(BF16)


def delta_kernel(*refs, n_kv, heads, key_heads, head_size, model_width, step_rows):
    count = n_kv - 1
    qk_own, v_own = refs[0], refs[1]
    qk_got, v_got = refs[2 : 2 + count], refs[2 + count : 2 + 2 * count]
    hist_q, hist_k, hist_v, taps_ref, decay_ref, fresh_ref, state_ref = refs[
        2 + 2 * count : 9 + 2 * count
    ]
    new_ref, readout_ref, scale_ref = refs[9 + 2 * count : 12 + 2 * count]
    q_scr, k_scr, v_scr, dot_scr, fade_scr, strength_scr = refs[12 + 2 * count :]
    key_cols = key_heads * head_size
    value_cols = heads * head_size
    repeat = heads // key_heads
    half = LANES // 2
    steps = q_scr.shape[1]

    def fold(values):
        return values.reshape(steps, step_rows, values.shape[-1])

    @pl.when(pl.program_id(0) == 0)
    def _():
        small = qk_own[:, 2 * key_cols :]
        for ref in qk_got:
            got = ref[:, 2 * key_cols :].astype(F32)
            small = small + got + pltpu.roll(got, half, 1)
        row_scale = lax.rsqrt(small[:, half - 1 : half] / model_width + EPSILON)
        scale_ref[...] = jnp.broadcast_to(row_scale, scale_ref.shape)
        small = small * row_scale
        strength = jax.nn.sigmoid(small[:, :heads])
        logits = small[:, heads : 2 * heads] + decay_ref[1:2, :]
        fade = jnp.exp(-jnp.exp(decay_ref[0:1, :]) * jax.nn.softplus(logits))
        fade = jnp.where(fresh_ref[...] > 0, 0.0, fade)

        def joined(own, gots, first, size):
            total = own[:, first : first + size]
            for ref in gots:
                total = total + ref[:, first : first + size].astype(F32)
            return total * row_scale

        for g in range(key_heads):
            first = g * head_size
            cols = slice(first, first + head_size)
            q = joined(qk_own, qk_got, first, head_size) * taps_ref[0:1, cols] + hist_q[:, cols]
            q = silu(q)
            q = q * lax.rsqrt(jnp.sum(q * q, axis=1, keepdims=True) + EPSILON)
            q = q * head_size ** (-0.5)
            k = joined(qk_own, qk_got, key_cols + first, head_size)
            k = silu(
                k * taps_ref[0:1, key_cols + first : key_cols + first + head_size]
                + hist_k[:, cols]
            )
            k = k * lax.rsqrt(jnp.sum(k * k, axis=1, keepdims=True) + EPSILON)
            q_scr[g] = fold(q)
            k_scr[g] = fold(k)
            dot_scr[g] = fold(
                jnp.broadcast_to(jnp.sum(q * k, axis=1, keepdims=True), q.shape)
            )
        for h in range(heads):
            first = h * head_size
            cols = slice(first, first + head_size)
            taps = taps_ref[0:1, 2 * key_cols + first : 2 * key_cols + first + head_size]
            v = silu(joined(v_own, v_got, first, head_size) * taps + hist_v[:, cols])
            v_scr[h] = fold(v)
            fade_scr[h] = fold(jnp.broadcast_to(fade[:, h : h + 1], v.shape))
            strength_scr[h] = fold(jnp.broadcast_to(strength[:, h : h + 1], v.shape))

    step = pl.program_id(0)
    for g in range(key_heads):
        q_cols = q_scr[g, step].T
        k_cols = k_scr[g, step].T
        for a in range(step_rows):
            k_wide = jnp.broadcast_to(k_cols[:, a : a + 1], (head_size, head_size))
            q_wide = jnp.broadcast_to(q_cols[:, a : a + 1], (head_size, head_size))
            for r in range(repeat):
                h = g * repeat + r
                state = state_ref[a, h]
                fade = fade_scr[h, step, a : a + 1, :]
                recalled = fade * jnp.sum(state * k_wide, axis=0, keepdims=True)
                update = strength_scr[h, step, a : a + 1, :] * (
                    v_scr[h, step, a : a + 1, :] - recalled
                )
                new_ref[a, h] = state * fade + k_wide * update
                read = fade * jnp.sum(state * q_wide, axis=0, keepdims=True)
                read = read + dot_scr[g, step, a : a + 1, :] * update
                readout_ref[a : a + 1, h * head_size : (h + 1) * head_size] = read


def gate_kernel(readout_ref, scale_ref, own_ref, *refs, n_kv, heads, head_size):
    got_refs, gain_ref, out_ref = refs[: n_kv - 1], refs[n_kv - 1], refs[n_kv]
    row_scale = scale_ref[:, 0:1]
    for h in range(heads):
        cols = slice(h * head_size, (h + 1) * head_size)
        gate_in = own_ref[:, cols]
        for ref in got_refs:
            gate_in = gate_in + ref[:, cols].astype(F32)
        gate_in = gate_in * row_scale
        read = readout_ref[:, cols]
        mean = jnp.sum(read * read, axis=1, keepdims=True) / head_size
        normed = read * lax.rsqrt(mean + EPSILON)
        out_ref[:, cols] = (normed * gain_ref[...].astype(F32) * silu(gate_in)).astype(BF16)


def mixer_kernel(*refs, n_kv, rows_block):
    w_ref, part_ref, send_ref = refs[n_kv : n_kv + 3]
    gated = jnp.concatenate([ref[...] for ref in refs[:n_kv]], axis=0)
    part = jnp.dot(gated, w_ref[...], preferred_element_type=F32)
    part_ref[...] = part
    send_ref[...] = part.astype(BF16)


def up_kernel(place, *refs, pieces, got, rows_block, n_kv):
    piece_refs = refs[:pieces]
    part_ref, got_refs = refs[pieces], refs[pieces + 1 : pieces + 1 + got]
    gain_ref, w_ref = refs[pieces + 1 + got : pieces + 3 + got]
    mixed_ref, squares_ref, own_ref = refs[pieces + 3 + got : pieces + 6 + got]
    out_refs = refs[pieces + 6 + got : pieces + 5 + got + n_kv]
    stream_ref = refs[pieces + 5 + got + n_kv]
    kv_place, tp_place = place[0], place[1]
    for m in range(pieces):
        width = piece_refs[m].shape[1]
        first = pl.multiple_of((tp_place ^ m) * width, width)
        for d in range(n_kv):
            row = pl.multiple_of((kv_place ^ d) * rows_block, rows_block)
            stream_ref[d * rows_block : (d + 1) * rows_block, pl.ds(first, width)] = piece_refs[m][
                pl.ds(row, rows_block), :
            ].astype(F32)
    total = part_ref[...]
    for ref in got_refs:
        total = total + ref[...].astype(F32)
    mixed = (stream_ref[...] + total).astype(BF16)
    mixed_ref[...] = mixed
    wide = mixed.astype(F32)
    squares_ref[...] = jnp.sum(wide * wide, axis=1, keepdims=True)
    scaled = (wide * gain_ref[...].astype(F32)).astype(BF16)
    part = jnp.dot(scaled, w_ref[...], preferred_element_type=F32)
    own_ref[...] = part[:rows_block]
    for d in range(1, n_kv):
        out_refs[d - 1][...] = part[d * rows_block : (d + 1) * rows_block].astype(BF16)


def hidden_kernel(*refs):
    total = refs[0][...]
    for ref in refs[1:-1]:
        total = total + ref[...].astype(F32)
    total = jnp.maximum(total, 0.0)
    refs[-1][...] = (total * total).astype(BF16)


def down_kernel(*refs, n_kv):
    w_ref, out_ref = refs[n_kv], refs[n_kv + 1]
    hidden = jnp.concatenate([ref[...] for ref in refs[:n_kv]], axis=0)
    out_ref[...] = jnp.dot(hidden, w_ref[...], preferred_element_type=F32)


def last_kernel(place, mixed_ref, scale_ref, own_ref, *refs, n_kv, rows_block):
    out_ref = refs[-1]
    kv_place = place[0]
    total = own_ref[...]
    for ref in refs[:-1]:
        total = total + ref[...].astype(F32)
    result = (mixed_ref[...].astype(F32) + total * scale_ref[...]).astype(BF16)
    for d in range(n_kv):
        row = pl.multiple_of((kv_place ^ d) * rows_block, rows_block)
        out_ref[pl.ds(row, rows_block), :] = result[d * rows_block : (d + 1) * rows_block]


def history_sum(history, weights, live_rows):
    live = jnp.where(live_rows[:, :, None], history.astype(F32), 0.0)
    return jnp.sum(live * weights.astype(F32)[None, :-1], axis=1)


SMEM_SPEC = pl.BlockSpec(memory_space=pltpu.SMEM)


def call_placed(body, outs, place, *args, scratch=(), name):
    return pl.pallas_call(
        body,
        out_shape=outs,
        in_specs=[SMEM_SPEC] + [pl.BlockSpec(memory_space=pltpu.VMEM)] * len(args),
        scratch_shapes=list(scratch),
        name=name,
        compiler_params=pltpu.CompilerParams(vmem_limit_bytes=48 * 1024 * 1024),
    )(place, *args)


def on_device(
    stream,
    lengths,
    delta_state,
    q_hist,
    k_hist,
    v_hist,
    norm_gain,
    w_query,
    w_key,
    w_value,
    w_gate,
    w_beta,
    w_decay,
    conv_query,
    conv_key,
    conv_value,
    decay_log,
    time_bias,
    out_gain,
    w_out,
    mlp_gain,
    w_up,
    w_down,
):
    n_kv, n_tp = lax.axis_size("kv"), lax.axis_size("tp")
    model_width = norm_gain.shape[0]
    block_cols = model_width // n_kv
    piece_cols = stream.shape[1]
    kv_place = lax.axis_index("kv")
    tp_place = lax.axis_index("tp")
    place = jnp.stack([kv_place, tp_place]).astype(jnp.int32)
    block_first = kv_place * block_cols
    rows, rows_block = stream.shape[0], delta_state.shape[0]
    heads, head_size = delta_state.shape[1], delta_state.shape[2]
    key_cols, value_cols = q_hist.shape[2], v_hist.shape[2]
    key_heads = key_cols // head_size
    taps_count = q_hist.shape[1] + 1
    count = n_kv - 1

    pieces = [stream] + exchange([stream] * n_tp, "tp")
    if piece_cols % LANES:
        order = tp_place ^ jnp.arange(n_tp)
        pieces = [
            jnp.take(jnp.stack(pieces), order, axis=0).transpose(1, 0, 2).reshape(rows, block_cols)
        ]
        piece_place = place * jnp.array([1, 0], jnp.int32)
    else:
        piece_place = place

    def own_block(vector):
        return lax.dynamic_slice_in_dim(vector, block_first, block_cols).reshape(1, block_cols)

    def own_heads(vector):
        return lax.dynamic_slice_in_dim(vector, tp_place * heads, heads)

    def own_small(weight):
        return lax.dynamic_slice(weight, (block_first, tp_place * heads), (block_cols, heads))

    def own_taps(weights, columns):
        return lax.dynamic_slice_in_dim(weights, tp_place * columns, columns, 1)

    w_small = jnp.concatenate([own_small(w_beta), own_small(w_decay)], axis=1)
    small_block = shape_of((rows_block, 2 * key_cols + LANES), BF16)
    outs = call_placed(
        functools.partial(
            query_key_kernel,
            pieces=len(pieces),
            rows_block=rows_block,
            n_kv=n_kv,
            model_width=model_width,
        ),
        [shape_of((rows, block_cols), BF16), shape_of((rows_block, 2 * key_cols + LANES), F32)]
        + [small_block] * count,
        piece_place,
        *pieces,
        own_block(norm_gain),
        w_query,
        w_key,
        w_small,
        name="query_key",
    )
    scaled, qk_own = outs[0], outs[1]
    qk_got = exchange([None] + list(outs[2:]), "kv")
    value_block = shape_of((rows_block, value_cols), BF16)
    outs = call(
        functools.partial(value_gate_kernel, rows_block=rows_block, n_kv=n_kv),
        [shape_of((rows_block, value_cols), F32)] * 2 + [value_block] * (2 * count),
        scaled,
        w_value,
        w_gate,
        name="value_gate",
    )
    v_own, gate_own = outs[0], outs[1]
    v_got = exchange([None] + list(outs[2 : 2 + count]), "kv")
    gate_got = exchange([None] + list(outs[2 + count :]), "kv")

    live_rows = (
        jnp.arange(taps_count - 1, dtype=jnp.int32)[None, :] >= (taps_count - lengths)[:, None]
    )
    taps_q, taps_k = own_taps(conv_query, key_cols), own_taps(conv_key, key_cols)
    taps_v = own_taps(conv_value, value_cols)
    hist_q = history_sum(q_hist, taps_q, live_rows)
    hist_k = history_sum(k_hist, taps_k, live_rows)
    hist_v = history_sum(v_hist, taps_v, live_rows)
    last_taps = jnp.concatenate([taps_q[-1:], taps_k[-1:], taps_v[-1:]], axis=1).astype(F32)
    decay_terms = jnp.stack([own_heads(decay_log), own_heads(time_bias)])
    fresh = (lengths == 1).astype(F32)[:, None]

    step_rows = 8
    steps = rows_block // step_rows
    whole = pl.BlockSpec(memory_space=pltpu.VMEM)
    state_spec = pl.BlockSpec(
        (step_rows, heads, head_size, head_size), lambda i: (i, 0, 0, 0)
    )
    new_state, readout, row_scale = pl.pallas_call(
        functools.partial(
            delta_kernel,
            n_kv=n_kv,
            heads=heads,
            key_heads=key_heads,
            head_size=head_size,
            model_width=model_width,
            step_rows=step_rows,
        ),
        grid=(steps,),
        in_specs=[whole] * (8 + 2 * count) + [state_spec],
        out_specs=[
            state_spec,
            pl.BlockSpec((step_rows, value_cols), lambda i: (i, 0)),
            pl.BlockSpec((rows_block, LANES), lambda i: (0, 0)),
        ],
        out_shape=[
            shape_of(delta_state.shape, F32),
            shape_of((rows_block, value_cols), F32),
            shape_of((rows_block, LANES), F32),
        ],
        scratch_shapes=[
            pltpu.VMEM((key_heads, steps, step_rows, head_size), F32),
            pltpu.VMEM((key_heads, steps, step_rows, head_size), F32),
            pltpu.VMEM((heads, steps, step_rows, head_size), F32),
            pltpu.VMEM((key_heads, steps, step_rows, head_size), F32),
            pltpu.VMEM((heads, steps, step_rows, head_size), F32),
            pltpu.VMEM((heads, steps, step_rows, head_size), F32),
        ],
        name="delta",
        compiler_params=pltpu.CompilerParams(
            vmem_limit_bytes=48 * 1024 * 1024, dimension_semantics=("arbitrary",)
        ),
    )(
        qk_own,
        v_own,
        *qk_got,
        *v_got,
        hist_q,
        hist_k,
        hist_v,
        last_taps,
        decay_terms,
        fresh,
        delta_state,
    )
    gated = call(
        functools.partial(gate_kernel, n_kv=n_kv, heads=heads, head_size=head_size),
        shape_of((rows_block, value_cols), BF16),
        readout,
        row_scale,
        gate_own,
        *gate_got,
        out_gain.reshape(1, head_size),
        name="gate",
    )
    gated_all = [gated] + exchange([gated] * n_kv, "kv")
    mixer_part, mixer_send = call(
        functools.partial(mixer_kernel, n_kv=n_kv, rows_block=rows_block),
        [shape_of((rows, block_cols), F32), shape_of((rows, block_cols), BF16)],
        *gated_all,
        w_out,
        name="mixer",
    )
    mixer_got = exchange([mixer_send] * n_tp, "tp")
    outs = call_placed(
        functools.partial(
            up_kernel,
            pieces=len(pieces),
            got=len(mixer_got),
            rows_block=rows_block,
            n_kv=n_kv,
        ),
        [
            shape_of((rows, block_cols), BF16),
            shape_of((rows, 1), F32),
            shape_of((rows_block, w_up.shape[1]), F32),
        ]
        + [shape_of((rows_block, w_up.shape[1]), BF16)] * count,
        piece_place,
        *pieces,
        mixer_part,
        *mixer_got,
        own_block(mlp_gain),
        w_up,
        scratch=[pltpu.VMEM((rows, block_cols), F32)],
        name="up",
    )
    mixed, squares, up_own = outs[0], outs[1], outs[2]
    up_got = exchange([None] + list(outs[3:]), "kv")
    square_blocks = squares.reshape(n_kv, rows_block)
    total_squares = square_blocks
    for m, got in enumerate(exchange([square_blocks] * n_kv, "kv"), 1):
        total_squares = total_squares + jnp.stack([got[d ^ m] for d in range(n_kv)])
    hidden = call(
        hidden_kernel,
        shape_of((rows_block, w_up.shape[1]), BF16),
        up_own,
        *up_got,
        name="hidden",
    )
    hidden_all = [hidden] + exchange([hidden] * n_kv, "kv")
    down_part = call(
        functools.partial(down_kernel, n_kv=n_kv),
        shape_of((rows, block_cols), F32),
        *hidden_all,
        w_down,
        name="down",
    )

    def piece(array, distance):
        return lax.dynamic_slice_in_dim(array, (tp_place ^ distance) * piece_cols, piece_cols, 1)

    down_got = exchange([None] + [piece(down_part, m).astype(BF16) for m in range(1, n_tp)], "tp")
    unit_squares = total_squares.reshape(rows, 1) / model_width + EPSILON
    result = call_placed(
        functools.partial(last_kernel, n_kv=n_kv, rows_block=rows_block),
        shape_of((rows, piece_cols), BF16),
        place,
        piece(mixed, 0),
        1.0 / unit_squares,
        piece(down_part, 0),
        *down_got,
        name="last",
    )
    return (result, new_state)


def solution(mesh):
    in_specs = (
        P("grp", ("kv", "tp")),
        P(("grp", "kv")),
        P(("grp", "kv"), "tp", None, None),
        P(("grp", "kv"), None, "tp"),
        P(("grp", "kv"), None, "tp"),
        P(("grp", "kv"), None, "tp"),
        P(),
        P("kv", "tp"),
        P("kv", "tp"),
        P("kv", "tp"),
        P("kv", "tp"),
        P(),
        P(),
        P(),
        P(),
        P(),
        P(),
        P(),
        P(),
        P("tp", "kv"),
        P(),
        P("kv", "tp"),
        P("tp", "kv"),
    )
    out_specs = (P("grp", ("kv", "tp")), P(("grp", "kv"), "tp", None, None))
    return jax.shard_map(
        on_device, mesh=mesh, in_specs=in_specs, out_specs=out_specs, check_vma=False
    )
```

```python
import functools

import jax
import jax.numpy as jnp
from jax import lax
from jax.experimental import pallas as pl
from jax.experimental.pallas import tpu as pltpu
from jax.sharding import PartitionSpec as P

EPSILON = 1e-06
LANES = 128
MIB = 1024 * 1024
F32 = jnp.float32
BF16 = jnp.bfloat16


def shape_of(shape, dtype):
    return jax.ShapeDtypeStruct(shape, dtype)


def call(body, outs, *args, scratch=(), name):
    return pl.pallas_call(
        body,
        out_shape=outs,
        scratch_shapes=list(scratch),
        name=name,
        compiler_params=pltpu.CompilerParams(vmem_limit_bytes=16 * MIB),
    )(*args)


def send(values, axis, distance):
    size = lax.axis_size(axis)
    return lax.ppermute(values, axis, [(i, i ^ distance) for i in range(size)])


def exchange(blocks, axis):
    got = {m: send(blocks[m], axis, m) for m in reversed(range(1, len(blocks)))}
    return [got[m] for m in range(1, len(blocks))]


def silu(values):
    return values * jax.nn.sigmoid(values)


def fetch_kernel(*refs, count):
    sources, targets, sems = refs[:count], refs[count : 2 * count], refs[2 * count]
    copies = []
    for index in range(count):
        source, target = sources[index], targets[index]
        if source.shape != target.shape:
            first = pl.multiple_of(lax.axis_index("kv") * target.shape[1], target.shape[1])
            source = source.at[:, pl.ds(first, target.shape[1])]
        copies.append(pltpu.make_async_copy(source, target, sems.at[index]))
    for copy in copies:
        copy.start()
    for copy in copies:
        copy.wait()


def fetch(*arrays, name, columns=None):
    shapes = [array.shape for array in arrays]
    if columns:
        shapes = [(shape[0], count) for shape, count in zip(shapes, columns)]
    return pl.pallas_call(
        functools.partial(fetch_kernel, count=len(arrays)),
        in_specs=[pl.BlockSpec(memory_space=pltpu.HBM)] * len(arrays),
        out_specs=[pl.BlockSpec(memory_space=pltpu.VMEM)] * len(arrays),
        out_shape=[pltpu.VMEM(shape, array.dtype) for shape, array in zip(shapes, arrays)],
        scratch_shapes=[pltpu.SemaphoreType.DMA((len(arrays),))],
        name=name,
        compiler_params=pltpu.CompilerParams(vmem_limit_bytes=MIB),
    )(*[pltpu.with_memory_space_constraint(array, pltpu.HBM) for array in arrays])


def project_kernel(*refs, pieces, rows_block, n_kv, heads, block_cols):
    piece_refs = refs[:pieces]
    gain_ref, w_query_ref, w_key_ref, w_value_ref, w_gate_ref, w_beta_ref, w_decay_ref = refs[
        pieces : pieces + 7
    ]
    own_ref, gate_own_ref = refs[pieces + 7 : pieces + 9]
    out_refs = refs[pieces + 9 : pieces + 8 + n_kv]
    gate_refs = refs[pieces + 8 + n_kv : pieces + 7 + 2 * n_kv]
    scaled_ref = refs[pieces + 7 + 2 * n_kv]
    kv_place, tp_place = lax.axis_index("kv"), lax.axis_index("tp")
    squares = [0.0] * n_kv
    for m in range(pieces):
        width = piece_refs[m].shape[1]
        first = pl.multiple_of((tp_place ^ m) * width if pieces > 1 else 0, LANES)
        gain_first = pl.multiple_of(kv_place * block_cols + first, LANES)
        gain = gain_ref[0:1, pl.ds(gain_first, width)].astype(F32)
        for d in range(n_kv):
            row = pl.multiple_of((kv_place ^ d) * rows_block, rows_block)
            wide = piece_refs[m][pl.ds(row, rows_block), :].astype(F32)
            squares[d] = squares[d] + jnp.sum(wide * wide, axis=1, keepdims=True)
            scaled_ref[d * rows_block : (d + 1) * rows_block, pl.ds(first, width)] = (
                wide * gain
            ).astype(BF16)
    scaled = scaled_ref[...]
    first = 0
    for w_ref in (w_query_ref, w_key_ref, w_value_ref):
        part = jnp.dot(scaled, w_ref[...], preferred_element_type=F32)
        cols = slice(first, first + w_ref.shape[1])
        first = first + w_ref.shape[1]
        own_ref[:, cols] = part[:rows_block]
        for d in range(1, n_kv):
            out_refs[d - 1][:, cols] = part[d * rows_block : (d + 1) * rows_block].astype(BF16)
    lane = lax.broadcasted_iota(jnp.int32, (scaled.shape[0], LANES), 1)
    total_heads = w_beta_ref.shape[0]

    def small_dot(w_ref, place):
        part = lax.dot_general(
            scaled, w_ref[...], (((1,), (1,)), ((), ())), preferred_element_type=F32
        )
        part = jnp.pad(part, ((0, 0), (0, LANES - total_heads)))
        return pltpu.roll(part, LANES + place - tp_place * heads, 1)

    small = jnp.where(lane < heads, small_dot(w_beta_ref, 0), small_dot(w_decay_ref, heads))
    lane = lane[:rows_block]
    half = LANES // 2
    for d in range(n_kv):
        block = small[d * rows_block : (d + 1) * rows_block]
        block = jnp.where(lane == half - 1, squares[d], block)
        if d == 0:
            own_ref[:, first:] = block
        else:
            high = block.astype(BF16)
            low = (block - high.astype(F32)).astype(BF16)
            out_refs[d - 1][:, first:] = jnp.where(
                lane < half, high.astype(F32), pltpu.roll(low.astype(F32), half, 1)
            ).astype(BF16)
    part = jnp.dot(scaled, w_gate_ref[...], preferred_element_type=F32)
    gate_own_ref[...] = part[:rows_block]
    for d in range(1, n_kv):
        gate_refs[d - 1][...] = part[d * rows_block : (d + 1) * rows_block].astype(BF16)


def history_kernel(lengths_ref, *refs):
    tp_place = lax.axis_index("tp")
    past, rows, _ = refs[0].shape
    row = lax.broadcasted_iota(jnp.int32, (rows, LANES), 0)
    lengths = jnp.zeros((rows, LANES), jnp.int32)
    for s in range(rows):
        lengths = jnp.where(row == s, lengths_ref[s], lengths)
    refs[9][...] = (lengths == 1).astype(F32)
    for hist_ref, taps_ref, out_ref in zip(refs[:3], refs[3:6], refs[6:9]):
        width = hist_ref.shape[2]
        taps = taps_ref[:, pl.ds(pl.multiple_of(tp_place * width, LANES), width)].astype(F32)
        total = 0.0
        for r in range(past):
            live = lengths[:, 0:1] >= past + 1 - r
            total = total + jnp.where(live, hist_ref[r].astype(F32), 0.0) * taps[r : r + 1]
        out_ref[...] = total


def delta_kernel(*refs, n_kv, heads, key_heads, head_size, model_width, step_rows):
    got_refs, refs = refs[1:n_kv], (refs[0],) + refs[n_kv:]
    own_ref, hist_q, hist_k, hist_v, fresh_ref, taps_q, taps_k, taps_v = refs[:8]
    decay_ref, bias_ref, state_ref, new_ref, readout_ref, scale_ref = refs[8:14]
    q_scr, k_scr, v_scr, dot_scr, fade_scr, strength_scr = refs[14:]
    key_cols = key_heads * head_size
    value_cols = heads * head_size
    repeat = heads // key_heads
    half = LANES // 2
    steps = q_scr.shape[1]
    tp_place = lax.axis_index("tp")

    def fold(values):
        return values.reshape(steps, step_rows, values.shape[-1])

    @pl.when(pl.program_id(0) == 0)
    def _():
        small_first = 2 * key_cols + value_cols
        small = own_ref[:, small_first:]
        for ref in got_refs:
            got = ref[:, small_first:].astype(F32)
            small = small + got + pltpu.roll(got, half, 1)
        row_scale = lax.rsqrt(small[:, half - 1 : half] / model_width + EPSILON)
        scale_ref[...] = jnp.broadcast_to(row_scale, scale_ref.shape)
        small = small * row_scale
        strength = jax.nn.sigmoid(small)
        to_decay = LANES + heads - tp_place * heads

        def by_head(ref):
            row = jnp.pad(ref[...], ((0, 7), (0, LANES - ref.shape[1])))
            return pltpu.roll(row, to_decay, 1)[0:1]

        logits = small + by_head(bias_ref)
        fade = jnp.exp(-jnp.exp(by_head(decay_ref)) * jax.nn.softplus(logits))
        fade = jnp.where(fresh_ref[...] > 0, 0.0, fade)

        def filtered(first, hist, taps_ref, head):
            cols = slice(first, first + head_size)
            total = own_ref[:, cols]
            for ref in got_refs:
                total = total + ref[:, cols].astype(F32)
            width = hist.shape[1]
            tap_first = pl.multiple_of(tp_place * width + head * head_size, LANES)
            taps = taps_ref[:, pl.ds(tap_first, head_size)].astype(F32)[-1:]
            past = hist[:, head * head_size : (head + 1) * head_size]
            return silu(total * row_scale * taps + past)

        for g in range(key_heads):
            q = filtered(g * head_size, hist_q, taps_q, g)
            q = q * lax.rsqrt(jnp.sum(q * q, axis=1, keepdims=True) + EPSILON)
            q = q * head_size ** (-0.5)
            k = filtered(key_cols + g * head_size, hist_k, taps_k, g)
            k = k * lax.rsqrt(jnp.sum(k * k, axis=1, keepdims=True) + EPSILON)
            q_scr[g] = fold(q)
            k_scr[g] = fold(k)
            dot_scr[g] = fold(jnp.broadcast_to(jnp.sum(q * k, axis=1, keepdims=True), q.shape))
        for h in range(heads):
            v = filtered(2 * key_cols + h * head_size, hist_v, taps_v, h)
            v_scr[h] = fold(v)
            fade_scr[h] = fold(jnp.broadcast_to(fade[:, heads + h : heads + h + 1], v.shape))
            strength_scr[h] = fold(jnp.broadcast_to(strength[:, h : h + 1], v.shape))

    step = pl.program_id(0)
    pair = repeat * head_size
    place = lax.broadcasted_iota(jnp.int32, (step_rows, pair), 0)
    nothing = jnp.zeros((step_rows, head_size), F32)
    for g in range(key_heads):
        group = range(g * repeat, (g + 1) * repeat)

        def wide(scr):
            return jnp.concatenate([scr[h, step] for h in group], axis=1)

        k, q = k_scr[g, step], q_scr[g, step]
        asked = jnp.concatenate([k, q], axis=0).astype(BF16)
        recalled, read = 0.0, 0.0
        for a in range(step_rows):
            row = step * step_rows + a
            state = jnp.concatenate([state_ref[row, h].astype(BF16) for h in group], axis=1)
            found = jnp.dot(asked, state, preferred_element_type=F32)
            recalled = recalled + jnp.where(place == a, found[:step_rows], 0.0)
            read = read + jnp.where(place == a, found[step_rows:], 0.0)
        fade = wide(fade_scr)
        update = wide(strength_scr) * (wide(v_scr) - fade * recalled)
        dots = jnp.concatenate([dot_scr[g, step]] * repeat, axis=1)
        readout_ref[:, g * pair : (g + 1) * pair] = fade * read + dots * update
        k_high = k.astype(BF16).astype(F32)
        keys = jnp.concatenate([k_high, k - k_high, k_high, nothing], axis=0).T.astype(BF16)
        high = update.astype(BF16).astype(F32)
        low = update - high
        for a in range(step_rows):
            row = step * step_rows + a
            high_a, low_a = jnp.where(place == a, high, 0.0), jnp.where(place == a, low, 0.0)
            rows = jnp.concatenate([high_a, high_a, low_a, low_a], axis=0).astype(BF16)
            added = jnp.dot(keys, rows, preferred_element_type=F32)
            for r, h in enumerate(group):
                fade_row = fade_scr[h, step, a : a + 1, :]
                new_ref[a, h] = (
                    state_ref[row, h] * fade_row + added[:, r * head_size : (r + 1) * head_size]
                )


def gate_kernel(readout_ref, scale_ref, own_ref, *refs, n_kv, heads, head_size):
    got_refs, gain_ref, out_ref = refs[: n_kv - 1], refs[n_kv - 1], refs[n_kv]
    row_scale = scale_ref[:, 0:1]
    for h in range(heads):
        cols = slice(h * head_size, (h + 1) * head_size)
        gate_in = own_ref[:, cols]
        for ref in got_refs:
            gate_in = gate_in + ref[:, cols].astype(F32)
        gate_in = gate_in * row_scale
        read = readout_ref[:, cols]
        mean = jnp.sum(read * read, axis=1, keepdims=True) / head_size
        normed = read * lax.rsqrt(mean + EPSILON)
        out_ref[:, cols] = (normed * gain_ref[...].astype(F32) * silu(gate_in)).astype(BF16)


def mixer_kernel(*refs, n_kv, rows_block):
    w_ref, part_ref, send_ref = refs[n_kv : n_kv + 3]
    gated = jnp.concatenate([ref[...] for ref in refs[:n_kv]], axis=0)
    part = jnp.dot(gated, w_ref[...], preferred_element_type=F32)
    part_ref[...] = part
    send_ref[...] = part.astype(BF16)


def up_kernel(*refs, pieces, got, rows_block, n_kv, block_cols):
    piece_refs = refs[:pieces]
    part_ref, got_refs = refs[pieces], refs[pieces + 1 : pieces + 1 + got]
    gain_ref, w_ref = refs[pieces + 1 + got : pieces + 3 + got]
    mixed_ref, squares_ref, own_ref = refs[pieces + 3 + got : pieces + 6 + got]
    out_refs = refs[pieces + 6 + got : pieces + 5 + got + n_kv]
    stream_ref = refs[pieces + 5 + got + n_kv]
    kv_place, tp_place = lax.axis_index("kv"), lax.axis_index("tp")
    for m in range(pieces):
        width = piece_refs[m].shape[1]
        first = pl.multiple_of((tp_place ^ m) * width if pieces > 1 else 0, LANES)
        for d in range(n_kv):
            row = pl.multiple_of((kv_place ^ d) * rows_block, rows_block)
            stream_ref[d * rows_block : (d + 1) * rows_block, pl.ds(first, width)] = piece_refs[m][
                pl.ds(row, rows_block), :
            ].astype(F32)
    total = part_ref[...]
    for ref in got_refs:
        total = total + ref[...].astype(F32)
    mixed = (stream_ref[...] + total).astype(BF16)
    wide = mixed.astype(F32)
    stream_ref[...] = wide
    if mixed_ref.shape[1] == block_cols:
        mixed_ref[...] = mixed
    else:
        width = mixed_ref.shape[1]
        mixed_ref[...] = stream_ref[:, pl.ds(pl.multiple_of(tp_place * width, LANES), width)].astype(
            BF16
        )
    squares = jnp.sum(wide * wide, axis=1, keepdims=True)
    squares_ref[...] = jnp.broadcast_to(squares, (squares.shape[0], LANES)).T[:8]
    gain = gain_ref[0:1, pl.ds(pl.multiple_of(kv_place * block_cols, LANES), block_cols)]
    scaled = (wide * gain.astype(F32)).astype(BF16)
    part = jnp.dot(scaled, w_ref[...], preferred_element_type=F32)
    own_ref[...] = part[:rows_block]
    for d in range(1, n_kv):
        out_refs[d - 1][...] = part[d * rows_block : (d + 1) * rows_block].astype(BF16)


def hidden_kernel(*refs):
    squares_ref, squares_out = refs[-3], refs[-1]
    squares_out[...] = squares_ref[...]
    total = refs[0][...]
    for ref in refs[1:-3]:
        total = total + ref[...].astype(F32)
    total = jnp.maximum(total, 0.0)
    refs[-2][...] = (total * total).astype(BF16)


def unit_factor(square_refs, rows_block, model_width):
    squares = square_refs[0][...]
    rows = squares.shape[1]
    block = lax.broadcasted_iota(jnp.int32, squares.shape, 1) // rows_block
    for m in range(1, len(square_refs)):
        got = square_refs[m][...]
        bit = 1
        while bit < len(square_refs):
            if m & bit:
                got = jnp.where(
                    (block & bit) == 0,
                    pltpu.roll(got, rows - bit * rows_block, 1),
                    pltpu.roll(got, bit * rows_block, 1),
                )
            bit *= 2
        squares = squares + got
    return (1.0 / (squares / model_width + EPSILON)).T[:, 0:1]


def down_kernel(*refs, n_kv, n_tp, rows_block, model_width):
    w_ref, own_ref = refs[n_kv], refs[2 * n_kv + 1]
    factor = unit_factor(refs[n_kv + 1 : 2 * n_kv + 1], rows_block, model_width)
    hidden = jnp.concatenate([ref[...] for ref in refs[:n_kv]], axis=0)
    part = jnp.dot(hidden, w_ref[...], preferred_element_type=F32) * factor
    if own_ref.shape == part.shape:
        own_ref[...] = part
        return
    send_refs, part_ref = refs[2 * n_kv + 2 : 2 * n_kv + 1 + n_tp], refs[2 * n_kv + 1 + n_tp]
    part_ref[...] = part
    width = own_ref.shape[1]
    for m in range(n_tp):
        first = pl.multiple_of((lax.axis_index("tp") ^ m) * width, LANES)
        piece = part_ref[:, pl.ds(first, width)]
        if m == 0:
            own_ref[...] = piece
        else:
            send_refs[m - 1][...] = piece.astype(BF16)


def last_kernel(mixed_ref, own_ref, *refs, n_kv, rows_block):
    out_ref = refs[-1]
    kv_place = lax.axis_index("kv")
    total = own_ref[...]
    for ref in refs[:-1]:
        total = total + ref[...].astype(F32)
    result = (mixed_ref[...].astype(F32) + total).astype(BF16)
    for d in range(n_kv):
        row = pl.multiple_of((kv_place ^ d) * rows_block, rows_block)
        out_ref[pl.ds(row, rows_block), :] = result[d * rows_block : (d + 1) * rows_block]


SMEM_SPEC = pl.BlockSpec(memory_space=pltpu.SMEM)
VMEM_SPEC = pl.BlockSpec(memory_space=pltpu.VMEM)


def on_device(
    stream,
    lengths,
    delta_state,
    q_hist,
    k_hist,
    v_hist,
    norm_gain,
    w_query,
    w_key,
    w_value,
    w_gate,
    w_beta,
    w_decay,
    conv_query,
    conv_key,
    conv_value,
    decay_log,
    time_bias,
    out_gain,
    w_out,
    mlp_gain,
    w_up,
    w_down,
):
    n_kv, n_tp = lax.axis_size("kv"), lax.axis_size("tp")
    model_width = norm_gain.shape[0]
    block_cols = model_width // n_kv
    piece_cols = stream.shape[1]
    aligned = piece_cols % LANES == 0
    tp_place = lax.axis_index("tp")
    rows, rows_block = stream.shape[0], delta_state.shape[0]
    heads, head_size = delta_state.shape[1], delta_state.shape[2]
    key_cols, value_cols = q_hist.shape[2], v_hist.shape[2]
    key_heads = key_cols // head_size
    count = n_kv - 1

    pieces = [stream] + exchange([stream] * n_tp, "tp")
    if not aligned:
        order = tp_place ^ jnp.arange(n_tp)
        pieces = [
            jnp.take(jnp.stack(pieces), order, axis=0).transpose(1, 0, 2).reshape(rows, block_cols)
        ]
    fetched = fetch(
        w_query,
        w_key,
        w_value,
        w_gate,
        w_beta.T,
        w_decay.T,
        name="fetch_input",
        columns=[w.shape[1] for w in (w_query, w_key, w_value, w_gate)] + [block_cols] * 2,
    )
    joined_cols = 2 * key_cols + value_cols + LANES
    outs = call(
        functools.partial(
            project_kernel,
            pieces=len(pieces),
            rows_block=rows_block,
            n_kv=n_kv,
            heads=heads,
            block_cols=block_cols,
        ),
        [shape_of((rows_block, joined_cols), F32), shape_of((rows_block, value_cols), F32)]
        + [shape_of((rows_block, joined_cols), BF16)] * count
        + [shape_of((rows_block, value_cols), BF16)] * count,
        *pieces,
        norm_gain.reshape(1, model_width),
        *fetched,
        scratch=[pltpu.VMEM((rows, block_cols), BF16)],
        name="project",
    )
    joined_own, gate_own = outs[0], outs[1]
    joined_got = exchange([None] + list(outs[2 : 2 + count]), "kv")
    gate_got = exchange([None] + list(outs[2 + count :]), "kv")

    hist = pl.pallas_call(
        history_kernel,
        in_specs=[SMEM_SPEC] + [VMEM_SPEC] * 6,
        out_shape=[
            shape_of((rows_block, width), F32) for width in (key_cols, key_cols, value_cols, LANES)
        ],
        name="history",
        compiler_params=pltpu.CompilerParams(vmem_limit_bytes=8 * MIB),
    )(
        lengths,
        *[array.transpose(1, 0, 2) for array in (q_hist, k_hist, v_hist)],
        conv_query,
        conv_key,
        conv_value,
    )
    state, w_down_near = fetch(delta_state, w_down, name="fetch_state")

    step_rows = 8
    steps = rows_block // step_rows
    state_spec = pl.BlockSpec(
        (step_rows, heads, head_size, head_size), lambda i: (i, 0, 0, 0)
    )
    new_state, readout, row_scale = pl.pallas_call(
        functools.partial(
            delta_kernel,
            n_kv=n_kv,
            heads=heads,
            key_heads=key_heads,
            head_size=head_size,
            model_width=model_width,
            step_rows=step_rows,
        ),
        grid=(steps,),
        in_specs=[VMEM_SPEC] * (n_kv + 10),
        out_specs=[
            state_spec,
            pl.BlockSpec((step_rows, value_cols), lambda i: (i, 0)),
            pl.BlockSpec((rows_block, LANES), lambda i: (0, 0)),
        ],
        out_shape=[
            shape_of(delta_state.shape, F32),
            shape_of((rows_block, value_cols), F32),
            shape_of((rows_block, LANES), F32),
        ],
        scratch_shapes=[
            pltpu.VMEM((key_heads, steps, step_rows, head_size), F32),
            pltpu.VMEM((key_heads, steps, step_rows, head_size), F32),
            pltpu.VMEM((heads, steps, step_rows, head_size), F32),
            pltpu.VMEM((key_heads, steps, step_rows, head_size), F32),
            pltpu.VMEM((heads, steps, step_rows, head_size), F32),
            pltpu.VMEM((heads, steps, step_rows, head_size), F32),
        ],
        name="delta",
        compiler_params=pltpu.CompilerParams(
            vmem_limit_bytes=24 * MIB, dimension_semantics=("arbitrary",)
        ),
    )(
        joined_own,
        *joined_got,
        *hist,
        conv_query,
        conv_key,
        conv_value,
        decay_log.reshape(1, -1),
        time_bias.reshape(1, -1),
        state,
    )
    gated = call(
        functools.partial(gate_kernel, n_kv=n_kv, heads=heads, head_size=head_size),
        shape_of((rows_block, value_cols), BF16),
        readout,
        row_scale,
        gate_own,
        *gate_got,
        out_gain.reshape(1, head_size),
        name="gate",
    )
    gated_all = [gated] + exchange([gated] * n_kv, "kv")
    mixer_part, mixer_send = call(
        functools.partial(mixer_kernel, n_kv=n_kv, rows_block=rows_block),
        [shape_of((rows, block_cols), F32), shape_of((rows, block_cols), BF16)],
        *gated_all,
        w_out,
        name="mixer",
    )
    mixer_got = exchange([mixer_send] * n_tp, "tp")
    unit_cols = w_up.shape[1]
    outs = call(
        functools.partial(
            up_kernel,
            pieces=len(pieces),
            got=len(mixer_got),
            rows_block=rows_block,
            n_kv=n_kv,
            block_cols=block_cols,
        ),
        [
            shape_of((rows, piece_cols if aligned else block_cols), BF16),
            shape_of((8, rows), F32),
            shape_of((rows_block, unit_cols), F32),
        ]
        + [shape_of((rows_block, unit_cols), BF16)] * count,
        *pieces,
        mixer_part,
        *mixer_got,
        mlp_gain.reshape(1, model_width),
        w_up,
        scratch=[pltpu.VMEM((rows, block_cols), F32)],
        name="up",
    )
    mixed, squares, up_own = outs[0], outs[1], outs[2]
    hidden, squares = call(
        hidden_kernel,
        [shape_of((rows_block, unit_cols), BF16), shape_of((8, rows), F32)],
        up_own,
        *exchange([None] + list(outs[3:]), "kv"),
        squares,
        name="hidden",
    )
    hidden_all = [hidden] + exchange([hidden] * n_kv, "kv")
    squares_all = [squares] + exchange([squares] * n_kv, "kv")

    def piece(array, distance):
        return lax.dynamic_slice_in_dim(array, (tp_place ^ distance) * piece_cols, piece_cols, 1)

    down = functools.partial(
        down_kernel, n_kv=n_kv, n_tp=n_tp, rows_block=rows_block, model_width=model_width
    )
    if aligned:
        outs = call(
            down,
            [shape_of((rows, piece_cols), F32)] + [shape_of((rows, piece_cols), BF16)] * (n_tp - 1),
            *hidden_all,
            w_down_near,
            *squares_all,
            scratch=[pltpu.VMEM((rows, block_cols), F32)],
            name="down",
        )
        mixed_own, down_own, down_send = mixed, outs[0], list(outs[1:])
    else:
        part = call(
            down,
            shape_of((rows, block_cols), F32),
            *hidden_all,
            w_down_near,
            *squares_all,
            name="down",
        )
        mixed_own, down_own = piece(mixed, 0), piece(part, 0)
        down_send = [piece(part, m).astype(BF16) for m in range(1, n_tp)]
    result = call(
        functools.partial(last_kernel, n_kv=n_kv, rows_block=rows_block),
        shape_of((rows, piece_cols), BF16),
        mixed_own,
        down_own,
        *exchange([None] + down_send, "tp"),
        name="last",
    )
    return (result, new_state)


def solution(mesh):
    in_specs = (
        P("grp", ("kv", "tp")),
        P(("grp", "kv")),
        P(("grp", "kv"), "tp", None, None),
        P(("grp", "kv"), None, "tp"),
        P(("grp", "kv"), None, "tp"),
        P(("grp", "kv"), None, "tp"),
        P(),
        P("kv", "tp"),
        P("kv", "tp"),
        P("kv", "tp"),
        P("kv", "tp"),
        P(),
        P(),
        P(),
        P(),
        P(),
        P(),
        P(),
        P(),
        P("tp", "kv"),
        P(),
        P("kv", "tp"),
        P("tp", "kv"),
    )
    out_specs = (P("grp", ("kv", "tp")), P(("grp", "kv"), "tp", None, None))
    return jax.shard_map(
        on_device, mesh=mesh, in_specs=in_specs, out_specs=out_specs, check_vma=False
    )
```

```python
import functools

import jax
import jax.numpy as jnp
from jax import lax
from jax.experimental import pallas as pl
from jax.experimental.pallas import tpu as pltpu
from jax.sharding import PartitionSpec as P

EPSILON = 1e-06
LANES = 128
MIB = 1024 * 1024
F32 = jnp.float32
BF16 = jnp.bfloat16


def shape_of(shape, dtype):
    return jax.ShapeDtypeStruct(shape, dtype)


def call(body, outs, *args, scratch=(), name):
    return pl.pallas_call(
        body,
        out_shape=outs,
        scratch_shapes=list(scratch),
        name=name,
        compiler_params=pltpu.CompilerParams(vmem_limit_bytes=16 * MIB),
    )(*args)


def send(values, axis, distance):
    size = lax.axis_size(axis)
    return lax.ppermute(values, axis, [(i, i ^ distance) for i in range(size)])


def exchange(blocks, axis):
    got = {m: send(blocks[m], axis, m) for m in reversed(range(1, len(blocks)))}
    return [got[m] for m in range(1, len(blocks))]


def silu(values):
    return values * jax.nn.sigmoid(values)


def fetch_kernel(*refs, count):
    sources, targets, sems = refs[:count], refs[count : 2 * count], refs[2 * count]
    copies = []
    for index in range(count):
        source, target = sources[index], targets[index]
        if source.shape != target.shape:
            first = pl.multiple_of(lax.axis_index("kv") * target.shape[1], target.shape[1])
            source = source.at[:, pl.ds(first, target.shape[1])]
        copies.append(pltpu.make_async_copy(source, target, sems.at[index]))
    for copy in copies:
        copy.start()
    for copy in copies:
        copy.wait()


def fetch(*arrays, name, columns=None):
    shapes = [array.shape for array in arrays]
    if columns:
        shapes = [(shape[0], count) for shape, count in zip(shapes, columns)]
    return pl.pallas_call(
        functools.partial(fetch_kernel, count=len(arrays)),
        in_specs=[pl.BlockSpec(memory_space=pltpu.HBM)] * len(arrays),
        out_specs=[pl.BlockSpec(memory_space=pltpu.VMEM)] * len(arrays),
        out_shape=[pltpu.VMEM(shape, array.dtype) for shape, array in zip(shapes, arrays)],
        scratch_shapes=[pltpu.SemaphoreType.DMA((len(arrays),))],
        name=name,
        compiler_params=pltpu.CompilerParams(vmem_limit_bytes=MIB),
    )(*[pltpu.with_memory_space_constraint(array, pltpu.HBM) for array in arrays])


def project_kernel(*refs, pieces, rows_block, n_kv, heads, block_cols):
    piece_refs = refs[:pieces]
    gain_ref, w_query_ref, w_key_ref, w_value_ref, w_beta_ref, w_decay_ref = refs[
        pieces : pieces + 6
    ]
    scaled_ref, own_ref = refs[pieces + 6 : pieces + 8]
    out_refs = refs[pieces + 8 :]
    kv_place, tp_place = lax.axis_index("kv"), lax.axis_index("tp")
    squares = [0.0] * n_kv
    for m in range(pieces):
        width = piece_refs[m].shape[1]
        first = pl.multiple_of((tp_place ^ m) * width if pieces > 1 else 0, LANES)
        gain_first = pl.multiple_of(kv_place * block_cols + first, LANES)
        gain = gain_ref[0:1, pl.ds(gain_first, width)].astype(F32)
        for d in range(n_kv):
            row = pl.multiple_of((kv_place ^ d) * rows_block, rows_block)
            wide = piece_refs[m][pl.ds(row, rows_block), :].astype(F32)
            squares[d] = squares[d] + jnp.sum(wide * wide, axis=1, keepdims=True)
            scaled_ref[d * rows_block : (d + 1) * rows_block, pl.ds(first, width)] = (
                wide * gain
            ).astype(BF16)
    scaled = scaled_ref[...]
    first = 0
    for w_ref in (w_query_ref, w_key_ref, w_value_ref):
        part = jnp.dot(scaled, w_ref[...], preferred_element_type=F32)
        cols = slice(first, first + w_ref.shape[1])
        first = first + w_ref.shape[1]
        own_ref[:, cols] = part[:rows_block]
        for d in range(1, n_kv):
            out_refs[d - 1][:, cols] = part[d * rows_block : (d + 1) * rows_block].astype(BF16)
    lane = lax.broadcasted_iota(jnp.int32, (scaled.shape[0], LANES), 1)
    total_heads = w_beta_ref.shape[0]

    def small_dot(w_ref, place):
        part = lax.dot_general(
            scaled, w_ref[...], (((1,), (1,)), ((), ())), preferred_element_type=F32
        )
        part = jnp.pad(part, ((0, 0), (0, LANES - total_heads)))
        return pltpu.roll(part, LANES + place - tp_place * heads, 1)

    small = jnp.where(lane < heads, small_dot(w_beta_ref, 0), small_dot(w_decay_ref, heads))
    lane = lane[:rows_block]
    half = LANES // 2
    for d in range(n_kv):
        block = small[d * rows_block : (d + 1) * rows_block]
        block = jnp.where(lane == half - 1, squares[d], block)
        if d == 0:
            own_ref[:, first:] = block
        else:
            high = block.astype(BF16)
            low = (block - high.astype(F32)).astype(BF16)
            out_refs[d - 1][:, first:] = jnp.where(
                lane < half, high.astype(F32), pltpu.roll(low.astype(F32), half, 1)
            ).astype(BF16)


def gate_project_kernel(scaled_ref, w_ref, after_ref, own_ref, *out_refs, rows_block):
    del after_ref
    part = jnp.dot(scaled_ref[...], w_ref[...], preferred_element_type=F32)
    own_ref[...] = part[:rows_block]
    for d, out_ref in enumerate(out_refs, 1):
        out_ref[...] = part[d * rows_block : (d + 1) * rows_block].astype(BF16)


def store_kernel(source, after_ref, target, done_ref, sems, *, chunks):
    done_ref[...] = after_ref[...]
    size = source.shape[0] // chunks
    copies = [
        pltpu.make_async_copy(
            source.at[pl.ds(i * size, size)], target.at[pl.ds(i * size, size)], sems.at[i]
        )
        for i in range(chunks)
    ]
    for copy in copies:
        copy.start()
    for copy in copies:
        copy.wait()


def history_kernel(lengths_ref, *refs):
    tp_place = lax.axis_index("tp")
    past, rows, _ = refs[0].shape
    row = lax.broadcasted_iota(jnp.int32, (rows, LANES), 0)
    lengths = jnp.zeros((rows, LANES), jnp.int32)
    for s in range(rows):
        lengths = jnp.where(row == s, lengths_ref[s], lengths)
    refs[9][...] = (lengths == 1).astype(F32)
    for hist_ref, taps_ref, out_ref in zip(refs[:3], refs[3:6], refs[6:9]):
        width = hist_ref.shape[2]
        taps = taps_ref[:, pl.ds(pl.multiple_of(tp_place * width, LANES), width)].astype(F32)
        total = 0.0
        for r in range(past):
            live = lengths[:, 0:1] >= past + 1 - r
            total = total + jnp.where(live, hist_ref[r].astype(F32), 0.0) * taps[r : r + 1]
        out_ref[...] = total


def delta_kernel(*refs, n_kv, heads, key_heads, head_size, model_width, step_rows):
    got_refs, refs = refs[1:n_kv], (refs[0],) + refs[n_kv:]
    own_ref, hist_q, hist_k, hist_v, fresh_ref, taps_q, taps_k, taps_v = refs[:8]
    decay_ref, bias_ref, state_ref, new_ref, readout_ref, scale_ref = refs[8:14]
    q_scr, k_scr, v_scr, dot_scr, fade_scr, strength_scr = refs[14:]
    key_cols = key_heads * head_size
    value_cols = heads * head_size
    repeat = heads // key_heads
    half = LANES // 2
    steps = q_scr.shape[1]
    tp_place = lax.axis_index("tp")

    def fold(values):
        return values.reshape(steps, step_rows, values.shape[-1])

    @pl.when(pl.program_id(0) == 0)
    def _():
        small_first = 2 * key_cols + value_cols
        small = own_ref[:, small_first:]
        for ref in got_refs:
            got = ref[:, small_first:].astype(F32)
            small = small + got + pltpu.roll(got, half, 1)
        row_scale = lax.rsqrt(small[:, half - 1 : half] / model_width + EPSILON)
        scale_ref[...] = jnp.broadcast_to(row_scale, scale_ref.shape)
        small = small * row_scale
        strength = jax.nn.sigmoid(small)
        to_decay = LANES + heads - tp_place * heads

        def by_head(ref):
            row = jnp.pad(ref[...], ((0, 7), (0, LANES - ref.shape[1])))
            return pltpu.roll(row, to_decay, 1)[0:1]

        logits = small + by_head(bias_ref)
        fade = jnp.exp(-jnp.exp(by_head(decay_ref)) * jax.nn.softplus(logits))
        fade = jnp.where(fresh_ref[...] > 0, 0.0, fade)

        def filtered(first, hist, taps_ref, head):
            cols = slice(first, first + head_size)
            total = own_ref[:, cols]
            for ref in got_refs:
                total = total + ref[:, cols].astype(F32)
            width = hist.shape[1]
            tap_first = pl.multiple_of(tp_place * width + head * head_size, LANES)
            taps = taps_ref[:, pl.ds(tap_first, head_size)].astype(F32)[-1:]
            past = hist[:, head * head_size : (head + 1) * head_size]
            return silu(total * row_scale * taps + past)

        for g in range(key_heads):
            q = filtered(g * head_size, hist_q, taps_q, g)
            q = q * lax.rsqrt(jnp.sum(q * q, axis=1, keepdims=True) + EPSILON)
            q = q * head_size ** (-0.5)
            k = filtered(key_cols + g * head_size, hist_k, taps_k, g)
            k = k * lax.rsqrt(jnp.sum(k * k, axis=1, keepdims=True) + EPSILON)
            q_scr[g] = fold(q)
            k_scr[g] = fold(k)
            dot_scr[g] = fold(jnp.broadcast_to(jnp.sum(q * k, axis=1, keepdims=True), q.shape))
        for h in range(heads):
            v = filtered(2 * key_cols + h * head_size, hist_v, taps_v, h)
            v_scr[h] = fold(v)
            fade_scr[h] = fold(jnp.broadcast_to(fade[:, heads + h : heads + h + 1], v.shape))
            strength_scr[h] = fold(jnp.broadcast_to(strength[:, h : h + 1], v.shape))

    step = pl.program_id(0)
    pair = repeat * head_size
    place = lax.broadcasted_iota(jnp.int32, (step_rows, pair), 0)
    def group(g):
        return range(g * repeat, (g + 1) * repeat)

    def wide(scr, g):
        return jnp.concatenate([scr[h, step] for h in group(g)], axis=1)

    def find(g, a, found):
        asked = jnp.concatenate([k_scr[g, step], q_scr[g, step]], axis=0).astype(BF16)
        row = step * step_rows + a
        state = jnp.concatenate([state_ref[row, h].astype(BF16) for h in group(g)], axis=1)
        now = jnp.dot(asked, state, preferred_element_type=F32)
        here = place == a
        return (
            found[0] + jnp.where(here, now[:step_rows], 0.0),
            found[1] + jnp.where(here, now[step_rows:], 0.0),
        )

    found = (0.0, 0.0)
    for a in range(step_rows):
        found = find(0, a, found)
    for g in range(key_heads):
        recalled, read = found
        found = (0.0, 0.0)
        k = k_scr[g, step]
        fade = wide(fade_scr, g)
        update = wide(strength_scr, g) * (wide(v_scr, g) - fade * recalled)
        dots = jnp.concatenate([dot_scr[g, step]] * repeat, axis=1)
        readout_ref[:, g * pair : (g + 1) * pair] = fade * read + dots * update
        k_columns = k.T
        for a in range(step_rows):
            row = step * step_rows + a
            k_wide = jnp.broadcast_to(k_columns[:, a : a + 1], (head_size, head_size))
            for r, h in enumerate(group(g)):
                fade_row = fade_scr[h, step, a : a + 1, :]
                update_row = update[a : a + 1, r * head_size : (r + 1) * head_size]
                new_ref[row, h] = state_ref[row, h] * fade_row + k_wide * update_row
            if g + 1 < key_heads:
                found = find(g + 1, a, found)


def gate_kernel(readout_ref, scale_ref, own_ref, *refs, n_kv, heads, head_size):
    got_refs, gain_ref, out_ref = refs[: n_kv - 1], refs[n_kv - 1], refs[n_kv]
    row_scale = scale_ref[:, 0:1]
    for h in range(heads):
        cols = slice(h * head_size, (h + 1) * head_size)
        gate_in = own_ref[:, cols]
        for ref in got_refs:
            gate_in = gate_in + ref[:, cols].astype(F32)
        gate_in = gate_in * row_scale
        read = readout_ref[:, cols]
        mean = jnp.sum(read * read, axis=1, keepdims=True) / head_size
        normed = read * lax.rsqrt(mean + EPSILON)
        out_ref[:, cols] = (normed * gain_ref[...].astype(F32) * silu(gate_in)).astype(BF16)


def mixer_kernel(*refs, n_kv):
    w_ref, part_ref, send_refs = refs[n_kv], refs[n_kv + 1], refs[n_kv + 2 :]
    gated = jnp.concatenate([ref[...] for ref in refs[:n_kv]], axis=0)
    part = jnp.dot(gated, w_ref[...], preferred_element_type=F32)
    part_ref[...] = part
    width = send_refs[0].shape[1]
    for index, ref in enumerate(send_refs):
        ref[...] = part[:, index * width : (index + 1) * width].astype(BF16)


def pair_kernel(part_ref, got_ref, *refs, first):
    out_ref = refs[-1]
    width = got_ref.shape[1]
    total = part_ref[:, first : first + width] + got_ref[...].astype(F32)
    out_ref[...] = total.astype(BF16)


def up_kernel(*refs, pieces, got, rows_block, n_kv, block_cols):
    piece_refs = refs[:pieces]
    part_ref, got_refs = refs[pieces], refs[pieces + 1 : pieces + 1 + got]
    gain_ref, w_ref = refs[pieces + 1 + got : pieces + 3 + got]
    mixed_ref, squares_ref, own_ref = refs[pieces + 3 + got : pieces + 6 + got]
    out_refs = refs[pieces + 6 + got : pieces + 5 + got + n_kv]
    stream_ref = refs[pieces + 5 + got + n_kv]
    kv_place, tp_place = lax.axis_index("kv"), lax.axis_index("tp")
    for m in range(pieces):
        width = piece_refs[m].shape[1]
        first = pl.multiple_of((tp_place ^ m) * width if pieces > 1 else 0, LANES)
        for d in range(n_kv):
            row = pl.multiple_of((kv_place ^ d) * rows_block, rows_block)
            stream_ref[d * rows_block : (d + 1) * rows_block, pl.ds(first, width)] = piece_refs[m][
                pl.ds(row, rows_block), :
            ].astype(F32)
    groups = block_cols // got_refs[0].shape[1]
    got_totals = []
    for index in range(groups):
        total = 0.0
        for ref in got_refs[index::groups]:
            total = total + ref[...].astype(F32)
        got_totals.append(total)
    total = part_ref[...] + jnp.concatenate(got_totals, axis=1)
    mixed = (stream_ref[...] + total).astype(BF16)
    wide = mixed.astype(F32)
    stream_ref[...] = wide
    if mixed_ref.shape[1] == block_cols:
        mixed_ref[...] = mixed
    else:
        width = mixed_ref.shape[1]
        mixed_ref[...] = stream_ref[:, pl.ds(pl.multiple_of(tp_place * width, LANES), width)].astype(
            BF16
        )
    squares = jnp.sum(wide * wide, axis=1, keepdims=True)
    squares_ref[...] = jnp.broadcast_to(squares, (squares.shape[0], LANES)).T[:8]
    gain = gain_ref[0:1, pl.ds(pl.multiple_of(kv_place * block_cols, LANES), block_cols)]
    scaled = (wide * gain.astype(F32)).astype(BF16)
    part = jnp.dot(scaled, w_ref[...], preferred_element_type=F32)
    own_ref[...] = part[:rows_block]
    for d in range(1, n_kv):
        out_refs[d - 1][...] = part[d * rows_block : (d + 1) * rows_block].astype(BF16)


def hidden_kernel(*refs):
    squares_ref, squares_out = refs[-3], refs[-1]
    squares_out[...] = squares_ref[...]
    total = refs[0][...]
    for ref in refs[1:-3]:
        total = total + ref[...].astype(F32)
    total = jnp.maximum(total, 0.0)
    refs[-2][...] = (total * total).astype(BF16)


def unit_factor(square_refs, rows_block, model_width):
    squares = square_refs[0][...]
    rows = squares.shape[1]
    block = lax.broadcasted_iota(jnp.int32, squares.shape, 1) // rows_block
    for m in range(1, len(square_refs)):
        got = square_refs[m][...]
        bit = 1
        while bit < len(square_refs):
            if m & bit:
                got = jnp.where(
                    (block & bit) == 0,
                    pltpu.roll(got, rows - bit * rows_block, 1),
                    pltpu.roll(got, bit * rows_block, 1),
                )
            bit *= 2
        squares = squares + got
    return (1.0 / (squares / model_width + EPSILON)).T[:, 0:1]


def down_kernel(*refs, n_kv, n_tp, rows_block, model_width):
    w_ref, own_ref = refs[n_kv], refs[2 * n_kv + 1]
    factor = unit_factor(refs[n_kv + 1 : 2 * n_kv + 1], rows_block, model_width)
    hidden = jnp.concatenate([ref[...] for ref in refs[:n_kv]], axis=0)
    part = jnp.dot(hidden, w_ref[...], preferred_element_type=F32) * factor
    if own_ref.shape == part.shape:
        own_ref[...] = part
        return
    send_refs, part_ref = refs[2 * n_kv + 2 : 2 * n_kv + 1 + n_tp], refs[2 * n_kv + 1 + n_tp]
    part_ref[...] = part
    width = own_ref.shape[1]
    for m in range(n_tp):
        first = pl.multiple_of((lax.axis_index("tp") ^ m) * width, LANES)
        piece = part_ref[:, pl.ds(first, width)]
        if m == 0:
            own_ref[...] = piece
        else:
            send_refs[m - 1][...] = piece.astype(BF16)


def last_kernel(mixed_ref, own_ref, *refs, n_kv, rows_block):
    out_ref = refs[-1]
    kv_place = lax.axis_index("kv")
    total = own_ref[...]
    for ref in refs[:-1]:
        total = total + ref[...].astype(F32)
    result = (mixed_ref[...].astype(F32) + total).astype(BF16)
    for d in range(n_kv):
        row = pl.multiple_of((kv_place ^ d) * rows_block, rows_block)
        out_ref[pl.ds(row, rows_block), :] = result[d * rows_block : (d + 1) * rows_block]


SMEM_SPEC = pl.BlockSpec(memory_space=pltpu.SMEM)
VMEM_SPEC = pl.BlockSpec(memory_space=pltpu.VMEM)


def on_device(
    stream,
    lengths,
    delta_state,
    q_hist,
    k_hist,
    v_hist,
    norm_gain,
    w_query,
    w_key,
    w_value,
    w_gate,
    w_beta,
    w_decay,
    conv_query,
    conv_key,
    conv_value,
    decay_log,
    time_bias,
    out_gain,
    w_out,
    mlp_gain,
    w_up,
    w_down,
):
    n_kv, n_tp = lax.axis_size("kv"), lax.axis_size("tp")
    model_width = norm_gain.shape[0]
    block_cols = model_width // n_kv
    piece_cols = stream.shape[1]
    aligned = piece_cols % LANES == 0
    tp_place = lax.axis_index("tp")
    rows, rows_block = stream.shape[0], delta_state.shape[0]
    heads, head_size = delta_state.shape[1], delta_state.shape[2]
    key_cols, value_cols = q_hist.shape[2], v_hist.shape[2]
    key_heads = key_cols // head_size
    count = n_kv - 1

    pieces = [stream] + exchange([stream] * n_tp, "tp")
    if not aligned:
        order = tp_place ^ jnp.arange(n_tp)
        pieces = [
            jnp.take(jnp.stack(pieces), order, axis=0).transpose(1, 0, 2).reshape(rows, block_cols)
        ]
    near = fetch(
        w_query,
        w_key,
        w_value,
        w_beta.T,
        w_decay.T,
        w_gate,
        *([stream] if aligned else []),
        name="fetch_input",
        columns=[w.shape[1] for w in (w_query, w_key, w_value)]
        + [block_cols] * 2
        + [value_cols]
        + [piece_cols] * aligned,
    )
    if aligned:
        pieces[0] = near[6]
    joined_cols = 2 * key_cols + value_cols + LANES
    outs = call(
        functools.partial(
            project_kernel,
            pieces=len(pieces),
            rows_block=rows_block,
            n_kv=n_kv,
            heads=heads,
            block_cols=block_cols,
        ),
        [shape_of((rows, block_cols), BF16), shape_of((rows_block, joined_cols), F32)]
        + [shape_of((rows_block, joined_cols), BF16)] * count,
        *pieces,
        norm_gain.reshape(1, model_width),
        *near[:5],
        name="project",
    )
    scaled, joined_own = outs[0], outs[1]
    joined_got = exchange([None] + list(outs[2:]), "kv")
    state, w_down_near = fetch(delta_state, w_down, name="fetch_state")
    outs = call(
        functools.partial(gate_project_kernel, rows_block=rows_block),
        [shape_of((rows_block, value_cols), F32)]
        + [shape_of((rows_block, value_cols), BF16)] * count,
        scaled,
        near[5],
        w_down_near,
        name="gate_project",
    )
    gate_own = outs[0]
    gate_got = exchange([None] + list(outs[1:]), "kv")

    hist = pl.pallas_call(
        history_kernel,
        in_specs=[SMEM_SPEC] + [VMEM_SPEC] * 6,
        out_shape=[
            shape_of((rows_block, width), F32) for width in (key_cols, key_cols, value_cols, LANES)
        ],
        name="history",
        compiler_params=pltpu.CompilerParams(vmem_limit_bytes=8 * MIB),
    )(
        lengths,
        *[array.transpose(1, 0, 2) for array in (q_hist, k_hist, v_hist)],
        conv_query,
        conv_key,
        conv_value,
    )

    step_rows = 8
    steps = rows_block // step_rows
    state_near, readout, row_scale = pl.pallas_call(
        functools.partial(
            delta_kernel,
            n_kv=n_kv,
            heads=heads,
            key_heads=key_heads,
            head_size=head_size,
            model_width=model_width,
            step_rows=step_rows,
        ),
        grid=(steps,),
        in_specs=[VMEM_SPEC] * (n_kv + 10),
        out_specs=[
            VMEM_SPEC,
            pl.BlockSpec((step_rows, value_cols), lambda i: (i, 0)),
            pl.BlockSpec((rows_block, LANES), lambda i: (0, 0)),
        ],
        out_shape=[
            pltpu.VMEM(delta_state.shape, F32),
            shape_of((rows_block, value_cols), F32),
            shape_of((rows_block, LANES), F32),
        ],
        input_output_aliases={n_kv + 9: 0},
        scratch_shapes=[
            pltpu.VMEM((key_heads, steps, step_rows, head_size), F32),
            pltpu.VMEM((key_heads, steps, step_rows, head_size), F32),
            pltpu.VMEM((heads, steps, step_rows, head_size), F32),
            pltpu.VMEM((key_heads, steps, step_rows, head_size), F32),
            pltpu.VMEM((heads, steps, step_rows, head_size), F32),
            pltpu.VMEM((heads, steps, step_rows, head_size), F32),
        ],
        name="delta",
        compiler_params=pltpu.CompilerParams(
            vmem_limit_bytes=8 * MIB, dimension_semantics=("arbitrary",)
        ),
    )(
        joined_own,
        *joined_got,
        *hist,
        conv_query,
        conv_key,
        conv_value,
        decay_log.reshape(1, -1),
        time_bias.reshape(1, -1),
        state,
    )
    gated = call(
        functools.partial(gate_kernel, n_kv=n_kv, heads=heads, head_size=head_size),
        shape_of((rows_block, value_cols), BF16),
        readout,
        row_scale,
        gate_own,
        *gate_got,
        out_gain.reshape(1, head_size),
        name="gate",
    )
    gated_all = [gated] + exchange([gated] * n_kv, "kv")
    halves = 2 if n_tp == 4 and block_cols % (2 * LANES) == 0 else 1
    half_block = shape_of((rows, block_cols // halves), BF16)
    outs = call(
        functools.partial(mixer_kernel, n_kv=n_kv),
        [shape_of((rows, block_cols), F32)] + [half_block] * halves,
        *gated_all,
        w_out,
        name="mixer",
    )
    mixer_part, mixer_send = outs[0], list(outs[1:])
    if halves == 2:
        mixer_got, before = [None] * 4, []
        for index, (near_step, far_step) in enumerate(((1, 2), (2, 1))):
            mixer_got[index] = send(mixer_send[index], "tp", near_step)
            pair = call(
                functools.partial(pair_kernel, first=index * block_cols // 2),
                half_block,
                mixer_part,
                mixer_got[index],
                *before,
                name=f"pair_{index}",
            )
            before = [pair]
            mixer_got[2 + index] = send(pair, "tp", far_step)
    else:
        mixer_got = exchange(mixer_send * n_tp, "tp")
    unit_cols = w_up.shape[1]
    outs = call(
        functools.partial(
            up_kernel,
            pieces=len(pieces),
            got=len(mixer_got),
            rows_block=rows_block,
            n_kv=n_kv,
            block_cols=block_cols,
        ),
        [
            shape_of((rows, piece_cols if aligned else block_cols), BF16),
            shape_of((8, rows), F32),
            shape_of((rows_block, unit_cols), F32),
        ]
        + [shape_of((rows_block, unit_cols), BF16)] * count,
        *pieces,
        mixer_part,
        *mixer_got,
        mlp_gain.reshape(1, model_width),
        w_up,
        scratch=[pltpu.VMEM((rows, block_cols), F32)],
        name="up",
    )
    mixed, squares, up_own = outs[0], outs[1], outs[2]
    chunks = 4
    new_state, squares = pl.pallas_call(
        functools.partial(store_kernel, chunks=chunks),
        in_specs=[VMEM_SPEC] * 2,
        out_specs=[pl.BlockSpec(memory_space=pltpu.HBM), VMEM_SPEC],
        out_shape=[shape_of(delta_state.shape, F32), shape_of(squares.shape, F32)],
        scratch_shapes=[pltpu.SemaphoreType.DMA((chunks,))],
        name="store_state",
        compiler_params=pltpu.CompilerParams(vmem_limit_bytes=MIB),
    )(state_near, squares)
    hidden, squares = call(
        hidden_kernel,
        [shape_of((rows_block, unit_cols), BF16), shape_of((8, rows), F32)],
        up_own,
        *exchange([None] + list(outs[3:]), "kv"),
        squares,
        name="hidden",
    )
    hidden_all = [hidden] + exchange([hidden] * n_kv, "kv")
    squares_all = [squares] + exchange([squares] * n_kv, "kv")

    def piece(array, distance):
        return lax.dynamic_slice_in_dim(array, (tp_place ^ distance) * piece_cols, piece_cols, 1)

    down = functools.partial(
        down_kernel, n_kv=n_kv, n_tp=n_tp, rows_block=rows_block, model_width=model_width
    )
    if aligned:
        outs = call(
            down,
            [shape_of((rows, piece_cols), F32)] + [shape_of((rows, piece_cols), BF16)] * (n_tp - 1),
            *hidden_all,
            w_down_near,
            *squares_all,
            scratch=[pltpu.VMEM((rows, block_cols), F32)],
            name="down",
        )
        mixed_own, down_own, down_send = mixed, outs[0], list(outs[1:])
    else:
        part = call(
            down,
            shape_of((rows, block_cols), F32),
            *hidden_all,
            w_down_near,
            *squares_all,
            name="down",
        )
        mixed_own, down_own = piece(mixed, 0), piece(part, 0)
        down_send = [piece(part, m).astype(BF16) for m in range(1, n_tp)]
    result = call(
        functools.partial(last_kernel, n_kv=n_kv, rows_block=rows_block),
        shape_of((rows, piece_cols), BF16),
        mixed_own,
        down_own,
        *exchange([None] + down_send, "tp"),
        name="last",
    )
    return (result, new_state)


def solution(mesh):
    in_specs = (
        P("grp", ("kv", "tp")),
        P(("grp", "kv")),
        P(("grp", "kv"), "tp", None, None),
        P(("grp", "kv"), None, "tp"),
        P(("grp", "kv"), None, "tp"),
        P(("grp", "kv"), None, "tp"),
        P(),
        P("kv", "tp"),
        P("kv", "tp"),
        P("kv", "tp"),
        P("kv", "tp"),
        P(),
        P(),
        P(),
        P(),
        P(),
        P(),
        P(),
        P(),
        P("tp", "kv"),
        P(),
        P("kv", "tp"),
        P("tp", "kv"),
    )
    out_specs = (P("grp", ("kv", "tp")), P(("grp", "kv"), "tp", None, None))
    return jax.shard_map(
        on_device, mesh=mesh, in_specs=in_specs, out_specs=out_specs, check_vma=False
    )
```

```python
import functools

import jax
import jax.numpy as jnp
from jax import lax
from jax.experimental import pallas as pl
from jax.experimental.pallas import tpu as pltpu
from jax.sharding import PartitionSpec as P

EPSILON = 1e-06
LANES = 128
MIB = 1024 * 1024
F32 = jnp.float32
BF16 = jnp.bfloat16


def shape_of(shape, dtype):
    return jax.ShapeDtypeStruct(shape, dtype)


def call(body, outs, *args, scratch=(), name):
    return pl.pallas_call(
        body,
        out_shape=outs,
        scratch_shapes=list(scratch),
        name=name,
        compiler_params=pltpu.CompilerParams(vmem_limit_bytes=16 * MIB),
    )(*args)


def send(values, axis, distance):
    size = lax.axis_size(axis)
    return lax.ppermute(values, axis, [(i, i ^ distance) for i in range(size)])


def exchange(blocks, axis):
    got = {m: send(blocks[m], axis, m) for m in reversed(range(1, len(blocks)))}
    return [got[m] for m in range(1, len(blocks))]


def silu(values):
    return values * jax.nn.sigmoid(values)


def fetch_kernel(*refs, count):
    sources, targets, sems = refs[:count], refs[count : 2 * count], refs[2 * count]
    copies = []
    for index in range(count):
        source, target = sources[index], targets[index]
        if source.shape != target.shape:
            first = pl.multiple_of(lax.axis_index("kv") * target.shape[1], target.shape[1])
            source = source.at[:, pl.ds(first, target.shape[1])]
        copies.append(pltpu.make_async_copy(source, target, sems.at[index]))
    for copy in copies:
        copy.start()
    for copy in copies:
        copy.wait()


def fetch(*arrays, name, columns=None):
    shapes = [array.shape for array in arrays]
    if columns:
        shapes = [(shape[0], count) for shape, count in zip(shapes, columns)]
    return pl.pallas_call(
        functools.partial(fetch_kernel, count=len(arrays)),
        in_specs=[pl.BlockSpec(memory_space=pltpu.HBM)] * len(arrays),
        out_specs=[pl.BlockSpec(memory_space=pltpu.VMEM)] * len(arrays),
        out_shape=[pltpu.VMEM(shape, array.dtype) for shape, array in zip(shapes, arrays)],
        scratch_shapes=[pltpu.SemaphoreType.DMA((len(arrays),))],
        name=name,
        compiler_params=pltpu.CompilerParams(vmem_limit_bytes=MIB),
    )(*[pltpu.with_memory_space_constraint(array, pltpu.HBM) for array in arrays])


def row_of(ref, index):
    values = ref[...].astype(F32)
    place = lax.broadcasted_iota(jnp.int32, values.shape, 0)
    return jnp.sum(jnp.where(place == index, values, 0.0), axis=0, keepdims=True)


def project_kernel(*refs, pieces, rows_block, n_kv, heads, block_cols):
    piece_refs = refs[:pieces]
    gain_ref, w_query_ref, w_key_ref, w_value_ref, w_beta_ref, w_decay_ref = refs[
        pieces : pieces + 6
    ]
    scaled_ref, own_ref = refs[pieces + 6 : pieces + 8]
    out_refs = refs[pieces + 8 :]
    kv_place, tp_place = lax.axis_index("kv"), lax.axis_index("tp")
    squares = [0.0] * n_kv
    for m in range(pieces):
        width = piece_refs[m].shape[1]
        first = pl.multiple_of((tp_place ^ m) * width if pieces > 1 else 0, LANES)
        gain_row = kv_place * (block_cols // LANES) + first // LANES
        gain = jnp.concatenate(
            [row_of(gain_ref, gain_row + j) for j in range(width // LANES)], axis=1
        )
        for d in range(n_kv):
            row = pl.multiple_of((kv_place ^ d) * rows_block, rows_block)
            wide = piece_refs[m][pl.ds(row, rows_block), :].astype(F32)
            squares[d] = squares[d] + jnp.sum(wide * wide, axis=1, keepdims=True)
            scaled_ref[d * rows_block : (d + 1) * rows_block, pl.ds(first, width)] = (
                wide * gain
            ).astype(BF16)
    scaled = scaled_ref[...]
    first = 0
    for w_ref in (w_query_ref, w_key_ref, w_value_ref):
        part = jnp.dot(scaled, w_ref[...], preferred_element_type=F32)
        cols = slice(first, first + w_ref.shape[1])
        first = first + w_ref.shape[1]
        own_ref[:, cols] = part[:rows_block]
        for d in range(1, n_kv):
            out_refs[d - 1][:, cols] = part[d * rows_block : (d + 1) * rows_block].astype(BF16)
    lane = lax.broadcasted_iota(jnp.int32, (scaled.shape[0], LANES), 1)
    total_heads = w_beta_ref.shape[0]

    def small_dot(w_ref, place):
        part = lax.dot_general(
            scaled, w_ref[...], (((1,), (1,)), ((), ())), preferred_element_type=F32
        )
        part = jnp.pad(part, ((0, 0), (0, LANES - total_heads)))
        return pltpu.roll(part, LANES + place - tp_place * heads, 1)

    small = jnp.where(lane < heads, small_dot(w_beta_ref, 0), small_dot(w_decay_ref, heads))
    lane = lane[:rows_block]
    half = LANES // 2
    for d in range(n_kv):
        block = small[d * rows_block : (d + 1) * rows_block]
        block = jnp.where(lane == half - 1, squares[d], block)
        if d == 0:
            own_ref[:, first:] = block
        else:
            high = block.astype(BF16)
            low = (block - high.astype(F32)).astype(BF16)
            out_refs[d - 1][:, first:] = jnp.where(
                lane < half, high.astype(F32), pltpu.roll(low.astype(F32), half, 1)
            ).astype(BF16)


def gate_project_kernel(scaled_ref, w_ref, after_ref, own_ref, *out_refs, rows_block):
    del after_ref
    part = jnp.dot(scaled_ref[...], w_ref[...], preferred_element_type=F32)
    own_ref[...] = part[:rows_block]
    for d, out_ref in enumerate(out_refs, 1):
        out_ref[...] = part[d * rows_block : (d + 1) * rows_block].astype(BF16)


def store_kernel(source, weight, after_ref, target, near_ref, done_ref, sems, *, chunks):
    done_ref[...] = after_ref[...]
    size = source.shape[0] // chunks
    copies = [
        pltpu.make_async_copy(
            source.at[pl.ds(i * size, size)], target.at[pl.ds(i * size, size)], sems.at[i]
        )
        for i in range(chunks)
    ]
    copies.append(pltpu.make_async_copy(weight, near_ref, sems.at[chunks]))
    for copy in copies:
        copy.start()
    for copy in copies:
        copy.wait()


def history_kernel(lengths_ref, *refs):
    tp_place = lax.axis_index("tp")
    past, rows, _ = refs[0].shape
    row = lax.broadcasted_iota(jnp.int32, (rows, LANES), 0)
    lengths = jnp.zeros((rows, LANES), jnp.int32)
    for s in range(rows):
        lengths = jnp.where(row == s, lengths_ref[s], lengths)
    refs[9][...] = (lengths == 1).astype(F32)
    for hist_ref, taps_ref, out_ref in zip(refs[:3], refs[3:6], refs[6:9]):
        width = hist_ref.shape[2]
        taps = taps_ref[:, pl.ds(pl.multiple_of(tp_place * width, LANES), width)].astype(F32)
        total = 0.0
        for r in range(past):
            live = lengths[:, 0:1] >= past + 1 - r
            total = total + jnp.where(live, hist_ref[r].astype(F32), 0.0) * taps[r : r + 1]
        out_ref[...] = total


def delta_kernel(*refs, n_kv, heads, key_heads, head_size, model_width, step_rows):
    got_refs, refs = refs[1:n_kv], (refs[0],) + refs[n_kv:]
    own_ref, hist_q, hist_k, hist_v, fresh_ref, taps_q, taps_k, taps_v = refs[:8]
    decay_ref, bias_ref, state_ref, new_ref, readout_ref, scale_ref = refs[8:14]
    q_scr, k_scr, v_scr, dot_scr, fade_scr, strength_scr = refs[14:]
    key_cols = key_heads * head_size
    value_cols = heads * head_size
    repeat = heads // key_heads
    half = LANES // 2
    steps = q_scr.shape[1]
    tp_place = lax.axis_index("tp")

    def fold(values):
        return values.reshape(steps, step_rows, values.shape[-1])

    @pl.when(pl.program_id(0) == 0)
    def _():
        small_first = 2 * key_cols + value_cols
        small = own_ref[:, small_first:]
        for ref in got_refs:
            got = ref[:, small_first:].astype(F32)
            small = small + got + pltpu.roll(got, half, 1)
        row_scale = lax.rsqrt(small[:, half - 1 : half] / model_width + EPSILON)
        scale_ref[...] = jnp.broadcast_to(row_scale, scale_ref.shape)
        small = small * row_scale
        strength = jax.nn.sigmoid(small)
        to_decay = LANES + heads - tp_place * heads

        def by_head(ref):
            row = jnp.pad(ref[...], ((0, 7), (0, LANES - ref.shape[1])))
            return pltpu.roll(row, to_decay, 1)[0:1]

        logits = small + by_head(bias_ref)
        fade = jnp.exp(-jnp.exp(by_head(decay_ref)) * jax.nn.softplus(logits))
        fade = jnp.where(fresh_ref[...] > 0, 0.0, fade)

        def filtered(first, hist, taps_ref, head):
            cols = slice(first, first + head_size)
            total = own_ref[:, cols]
            for ref in got_refs:
                total = total + ref[:, cols].astype(F32)
            width = hist.shape[1]
            tap_first = pl.multiple_of(tp_place * width + head * head_size, LANES)
            taps = taps_ref[:, pl.ds(tap_first, head_size)].astype(F32)[-1:]
            past = hist[:, head * head_size : (head + 1) * head_size]
            return silu(total * row_scale * taps + past)

        for g in range(key_heads):
            q = filtered(g * head_size, hist_q, taps_q, g)
            q = q * lax.rsqrt(jnp.sum(q * q, axis=1, keepdims=True) + EPSILON)
            q = q * head_size ** (-0.5)
            k = filtered(key_cols + g * head_size, hist_k, taps_k, g)
            k = k * lax.rsqrt(jnp.sum(k * k, axis=1, keepdims=True) + EPSILON)
            q_scr[g] = fold(q)
            k_scr[g] = fold(k)
            dot_scr[g] = fold(jnp.broadcast_to(jnp.sum(q * k, axis=1, keepdims=True), q.shape))
        for h in range(heads):
            v = filtered(2 * key_cols + h * head_size, hist_v, taps_v, h)
            v_scr[h] = fold(v)
            fade_scr[h] = fold(jnp.broadcast_to(fade[:, heads + h : heads + h + 1], v.shape))
            strength_scr[h] = fold(jnp.broadcast_to(strength[:, h : h + 1], v.shape))

    step = pl.program_id(0)
    pair = repeat * head_size
    place = lax.broadcasted_iota(jnp.int32, (step_rows, pair), 0)
    def group(g):
        return range(g * repeat, (g + 1) * repeat)

    def wide(scr, g):
        return jnp.concatenate([scr[h, step] for h in group(g)], axis=1)

    def find(g, a, found):
        asked = jnp.concatenate([k_scr[g, step], q_scr[g, step]], axis=0).astype(BF16)
        row = step * step_rows + a
        state = jnp.concatenate([state_ref[row, h].astype(BF16) for h in group(g)], axis=1)
        now = jnp.dot(asked, state, preferred_element_type=F32)
        here = place == a
        return (
            found[0] + jnp.where(here, now[:step_rows], 0.0),
            found[1] + jnp.where(here, now[step_rows:], 0.0),
        )

    found = (0.0, 0.0)
    for a in range(step_rows):
        found = find(0, a, found)
    for g in range(key_heads):
        recalled, read = found
        found = (0.0, 0.0)
        k = k_scr[g, step]
        fade = wide(fade_scr, g)
        update = wide(strength_scr, g) * (wide(v_scr, g) - fade * recalled)
        dots = jnp.concatenate([dot_scr[g, step]] * repeat, axis=1)
        readout_ref[:, g * pair : (g + 1) * pair] = fade * read + dots * update
        if g + 1 < key_heads:
            for a in range(step_rows):
                found = find(g + 1, a, found)
        k_columns = k.T
        for a in range(step_rows):
            row = step * step_rows + a
            k_wide = jnp.broadcast_to(k_columns[:, a : a + 1], (head_size, head_size))
            for r, h in enumerate(group(g)):
                fade_row = fade_scr[h, step, a : a + 1, :]
                update_row = update[a : a + 1, r * head_size : (r + 1) * head_size]
                new_ref[row, h] = state_ref[row, h] * fade_row + k_wide * update_row


def gate_kernel(readout_ref, scale_ref, own_ref, *refs, n_kv, heads, head_size):
    got_refs, gain_ref, out_ref = refs[: n_kv - 1], refs[n_kv - 1], refs[n_kv]
    row_scale = scale_ref[:, 0:1]
    for h in range(heads):
        cols = slice(h * head_size, (h + 1) * head_size)
        gate_in = own_ref[:, cols]
        for ref in got_refs:
            gate_in = gate_in + ref[:, cols].astype(F32)
        gate_in = gate_in * row_scale
        read = readout_ref[:, cols]
        mean = jnp.sum(read * read, axis=1, keepdims=True) / head_size
        normed = read * lax.rsqrt(mean + EPSILON)
        out_ref[:, cols] = (normed * gain_ref[...].astype(F32) * silu(gate_in)).astype(BF16)


def mixer_kernel(*refs, n_kv):
    w_ref, part_ref, send_refs = refs[n_kv], refs[n_kv + 1], refs[n_kv + 2 :]
    gated = jnp.concatenate([ref[...] for ref in refs[:n_kv]], axis=0)
    part = jnp.dot(gated, w_ref[...], preferred_element_type=F32)
    part_ref[...] = part
    width = send_refs[0].shape[1]
    for index, ref in enumerate(send_refs):
        ref[...] = part[:, index * width : (index + 1) * width].astype(BF16)


def pair_kernel(part_ref, got_ref, *refs, first):
    out_ref = refs[-1]
    width = got_ref.shape[1]
    total = part_ref[:, first : first + width] + got_ref[...].astype(F32)
    out_ref[...] = total.astype(BF16)


def up_kernel(*refs, pieces, got, rows_block, n_kv, block_cols):
    piece_refs = refs[:pieces]
    part_ref, got_refs = refs[pieces], refs[pieces + 1 : pieces + 1 + got]
    gain_ref, w_ref = refs[pieces + 1 + got : pieces + 3 + got]
    mixed_ref, squares_ref, own_ref = refs[pieces + 3 + got : pieces + 6 + got]
    out_refs = refs[pieces + 6 + got : pieces + 5 + got + n_kv]
    stream_ref = refs[pieces + 5 + got + n_kv]
    kv_place, tp_place = lax.axis_index("kv"), lax.axis_index("tp")
    for m in range(pieces):
        width = piece_refs[m].shape[1]
        first = pl.multiple_of((tp_place ^ m) * width if pieces > 1 else 0, LANES)
        for d in range(n_kv):
            row = pl.multiple_of((kv_place ^ d) * rows_block, rows_block)
            stream_ref[d * rows_block : (d + 1) * rows_block, pl.ds(first, width)] = piece_refs[m][
                pl.ds(row, rows_block), :
            ].astype(F32)
    groups = block_cols // got_refs[0].shape[1]
    got_totals = []
    for index in range(groups):
        total = 0.0
        for ref in got_refs[index::groups]:
            total = total + ref[...].astype(F32)
        got_totals.append(total)
    total = part_ref[...] + jnp.concatenate(got_totals, axis=1)
    mixed = (stream_ref[...] + total).astype(BF16)
    wide = mixed.astype(F32)
    stream_ref[...] = wide
    if mixed_ref.shape[1] == block_cols:
        mixed_ref[...] = mixed
    else:
        width = mixed_ref.shape[1]
        mixed_ref[...] = stream_ref[:, pl.ds(pl.multiple_of(tp_place * width, LANES), width)].astype(
            BF16
        )
    squares = jnp.sum(wide * wide, axis=1, keepdims=True)
    squares_ref[...] = jnp.broadcast_to(squares, (squares.shape[0], LANES)).T[:8]
    gain = gain_ref[0:1, pl.ds(pl.multiple_of(kv_place * block_cols, LANES), block_cols)]
    scaled = (wide * gain.astype(F32)).astype(BF16)
    part = jnp.dot(scaled, w_ref[...], preferred_element_type=F32)
    own_ref[...] = part[:rows_block]
    for d in range(1, n_kv):
        out_refs[d - 1][...] = part[d * rows_block : (d + 1) * rows_block].astype(BF16)


def hidden_kernel(*refs):
    squares_ref, squares_out = refs[-3], refs[-1]
    squares_out[...] = squares_ref[...]
    total = refs[0][...]
    for ref in refs[1:-3]:
        total = total + ref[...].astype(F32)
    total = jnp.maximum(total, 0.0)
    refs[-2][...] = (total * total).astype(BF16)


def unit_factor(square_refs, rows_block, model_width):
    squares = square_refs[0][...]
    rows = squares.shape[1]
    block = lax.broadcasted_iota(jnp.int32, squares.shape, 1) // rows_block
    for m in range(1, len(square_refs)):
        got = square_refs[m][...]
        bit = 1
        while bit < len(square_refs):
            if m & bit:
                got = jnp.where(
                    (block & bit) == 0,
                    pltpu.roll(got, rows - bit * rows_block, 1),
                    pltpu.roll(got, bit * rows_block, 1),
                )
            bit *= 2
        squares = squares + got
    return (1.0 / (squares / model_width + EPSILON)).T[:, 0:1]


def down_kernel(*refs, n_kv, n_tp, rows_block, model_width):
    w_ref, own_ref = refs[n_kv], refs[2 * n_kv + 1]
    factor = unit_factor(refs[n_kv + 1 : 2 * n_kv + 1], rows_block, model_width)
    hidden = jnp.concatenate([ref[...] for ref in refs[:n_kv]], axis=0)
    part = jnp.dot(hidden, w_ref[...], preferred_element_type=F32) * factor
    if own_ref.shape == part.shape:
        own_ref[...] = part
        return
    send_refs, part_ref = refs[2 * n_kv + 2 : 2 * n_kv + 1 + n_tp], refs[2 * n_kv + 1 + n_tp]
    part_ref[...] = part
    width = own_ref.shape[1]
    for m in range(n_tp):
        first = pl.multiple_of((lax.axis_index("tp") ^ m) * width, LANES)
        piece = part_ref[:, pl.ds(first, width)]
        if m == 0:
            own_ref[...] = piece
        else:
            send_refs[m - 1][...] = piece.astype(BF16)


def last_kernel(mixed_ref, own_ref, *refs, n_kv, rows_block):
    out_ref = refs[-1]
    kv_place = lax.axis_index("kv")
    total = own_ref[...]
    for ref in refs[:-1]:
        total = total + ref[...].astype(F32)
    result = (mixed_ref[...].astype(F32) + total).astype(BF16)
    for d in range(n_kv):
        row = pl.multiple_of((kv_place ^ d) * rows_block, rows_block)
        out_ref[pl.ds(row, rows_block), :] = result[d * rows_block : (d + 1) * rows_block]


SMEM_SPEC = pl.BlockSpec(memory_space=pltpu.SMEM)
VMEM_SPEC = pl.BlockSpec(memory_space=pltpu.VMEM)


def on_device(
    stream,
    lengths,
    delta_state,
    q_hist,
    k_hist,
    v_hist,
    norm_gain,
    w_query,
    w_key,
    w_value,
    w_gate,
    w_beta,
    w_decay,
    conv_query,
    conv_key,
    conv_value,
    decay_log,
    time_bias,
    out_gain,
    w_out,
    mlp_gain,
    w_up,
    w_down,
):
    n_kv, n_tp = lax.axis_size("kv"), lax.axis_size("tp")
    model_width = norm_gain.shape[0]
    block_cols = model_width // n_kv
    piece_cols = stream.shape[1]
    aligned = piece_cols % LANES == 0
    tp_place = lax.axis_index("tp")
    rows, rows_block = stream.shape[0], delta_state.shape[0]
    heads, head_size = delta_state.shape[1], delta_state.shape[2]
    key_cols, value_cols = q_hist.shape[2], v_hist.shape[2]
    key_heads = key_cols // head_size
    count = n_kv - 1

    pieces = [stream] + exchange([stream] * n_tp, "tp")
    if not aligned:
        order = tp_place ^ jnp.arange(n_tp)
        pieces = [
            jnp.take(jnp.stack(pieces), order, axis=0).transpose(1, 0, 2).reshape(rows, block_cols)
        ]
    near = fetch(
        w_query,
        w_key,
        w_value,
        w_beta.T,
        w_decay.T,
        w_gate,
        norm_gain.reshape(model_width // LANES, LANES),
        *([stream] if aligned else []),
        name="fetch_input",
        columns=[w.shape[1] for w in (w_query, w_key, w_value)]
        + [block_cols] * 2
        + [value_cols, LANES]
        + [piece_cols] * aligned,
    )
    if aligned:
        pieces[0] = near[7]
    joined_cols = 2 * key_cols + value_cols + LANES
    outs = call(
        functools.partial(
            project_kernel,
            pieces=len(pieces),
            rows_block=rows_block,
            n_kv=n_kv,
            heads=heads,
            block_cols=block_cols,
        ),
        [shape_of((rows, block_cols), BF16), shape_of((rows_block, joined_cols), F32)]
        + [shape_of((rows_block, joined_cols), BF16)] * count,
        *pieces,
        near[6],
        *near[:5],
        name="project",
    )
    scaled, joined_own = outs[0], outs[1]
    joined_got = exchange([None] + list(outs[2:]), "kv")
    (state,) = fetch(delta_state, name="fetch_state")
    outs = call(
        functools.partial(gate_project_kernel, rows_block=rows_block),
        [shape_of((rows_block, value_cols), F32)]
        + [shape_of((rows_block, value_cols), BF16)] * count,
        scaled,
        near[5],
        state,
        name="gate_project",
    )
    gate_own = outs[0]
    gate_got = exchange([None] + list(outs[1:]), "kv")

    hist = pl.pallas_call(
        history_kernel,
        in_specs=[SMEM_SPEC] + [VMEM_SPEC] * 6,
        out_shape=[
            shape_of((rows_block, width), F32) for width in (key_cols, key_cols, value_cols, LANES)
        ],
        name="history",
        compiler_params=pltpu.CompilerParams(vmem_limit_bytes=8 * MIB),
    )(
        lengths,
        *[array.transpose(1, 0, 2) for array in (q_hist, k_hist, v_hist)],
        conv_query,
        conv_key,
        conv_value,
    )

    step_rows = 8
    steps = rows_block // step_rows
    state_near, readout, row_scale = pl.pallas_call(
        functools.partial(
            delta_kernel,
            n_kv=n_kv,
            heads=heads,
            key_heads=key_heads,
            head_size=head_size,
            model_width=model_width,
            step_rows=step_rows,
        ),
        grid=(steps,),
        in_specs=[VMEM_SPEC] * (n_kv + 10),
        out_specs=[
            VMEM_SPEC,
            pl.BlockSpec((step_rows, value_cols), lambda i: (i, 0)),
            pl.BlockSpec((rows_block, LANES), lambda i: (0, 0)),
        ],
        out_shape=[
            pltpu.VMEM(delta_state.shape, F32),
            shape_of((rows_block, value_cols), F32),
            shape_of((rows_block, LANES), F32),
        ],
        input_output_aliases={n_kv + 9: 0},
        scratch_shapes=[
            pltpu.VMEM((key_heads, steps, step_rows, head_size), F32),
            pltpu.VMEM((key_heads, steps, step_rows, head_size), F32),
            pltpu.VMEM((heads, steps, step_rows, head_size), F32),
            pltpu.VMEM((key_heads, steps, step_rows, head_size), F32),
            pltpu.VMEM((heads, steps, step_rows, head_size), F32),
            pltpu.VMEM((heads, steps, step_rows, head_size), F32),
        ],
        name="delta",
        compiler_params=pltpu.CompilerParams(
            vmem_limit_bytes=8 * MIB, dimension_semantics=("arbitrary",)
        ),
    )(
        joined_own,
        *joined_got,
        *hist,
        conv_query,
        conv_key,
        conv_value,
        decay_log.reshape(1, -1),
        time_bias.reshape(1, -1),
        state,
    )
    gated = call(
        functools.partial(gate_kernel, n_kv=n_kv, heads=heads, head_size=head_size),
        shape_of((rows_block, value_cols), BF16),
        readout,
        row_scale,
        gate_own,
        *gate_got,
        out_gain.reshape(1, head_size),
        name="gate",
    )
    gated_all = [gated] + exchange([gated] * n_kv, "kv")
    halves = 2 if n_tp == 4 and block_cols % (2 * LANES) == 0 else 1
    half_block = shape_of((rows, block_cols // halves), BF16)
    outs = call(
        functools.partial(mixer_kernel, n_kv=n_kv),
        [shape_of((rows, block_cols), F32)] + [half_block] * halves,
        *gated_all,
        w_out,
        name="mixer",
    )
    mixer_part, mixer_send = outs[0], list(outs[1:])
    if halves == 2:
        mixer_got, before = [None] * 4, []
        for index, (near_step, far_step) in enumerate(((1, 2), (2, 1))):
            mixer_got[index] = send(mixer_send[index], "tp", near_step)
            pair = call(
                functools.partial(pair_kernel, first=index * block_cols // 2),
                half_block,
                mixer_part,
                mixer_got[index],
                *before,
                name=f"pair_{index}",
            )
            before = [pair]
            mixer_got[2 + index] = send(pair, "tp", far_step)
    else:
        mixer_got = exchange(mixer_send * n_tp, "tp")
    unit_cols = w_up.shape[1]
    outs = call(
        functools.partial(
            up_kernel,
            pieces=len(pieces),
            got=len(mixer_got),
            rows_block=rows_block,
            n_kv=n_kv,
            block_cols=block_cols,
        ),
        [
            shape_of((rows, piece_cols if aligned else block_cols), BF16),
            shape_of((8, rows), F32),
            shape_of((rows_block, unit_cols), F32),
        ]
        + [shape_of((rows_block, unit_cols), BF16)] * count,
        *pieces,
        mixer_part,
        *mixer_got,
        mlp_gain.reshape(1, model_width),
        w_up,
        scratch=[pltpu.VMEM((rows, block_cols), F32)],
        name="up",
    )
    mixed, squares, up_own = outs[0], outs[1], outs[2]
    chunks = 4
    new_state, w_down_near, squares = pl.pallas_call(
        functools.partial(store_kernel, chunks=chunks),
        in_specs=[VMEM_SPEC, pl.BlockSpec(memory_space=pltpu.HBM), VMEM_SPEC],
        out_specs=[pl.BlockSpec(memory_space=pltpu.HBM), VMEM_SPEC, VMEM_SPEC],
        out_shape=[
            shape_of(delta_state.shape, F32),
            pltpu.VMEM(w_down.shape, BF16),
            shape_of(squares.shape, F32),
        ],
        scratch_shapes=[pltpu.SemaphoreType.DMA((chunks + 1,))],
        name="store_state",
        compiler_params=pltpu.CompilerParams(vmem_limit_bytes=MIB),
    )(state_near, pltpu.with_memory_space_constraint(w_down, pltpu.HBM), squares)
    hidden, squares = call(
        hidden_kernel,
        [shape_of((rows_block, unit_cols), BF16), shape_of((8, rows), F32)],
        up_own,
        *exchange([None] + list(outs[3:]), "kv"),
        squares,
        name="hidden",
    )
    hidden_all = [hidden] + exchange([hidden] * n_kv, "kv")
    squares_all = [squares] + exchange([squares] * n_kv, "kv")

    def piece(array, distance):
        return lax.dynamic_slice_in_dim(array, (tp_place ^ distance) * piece_cols, piece_cols, 1)

    down = functools.partial(
        down_kernel, n_kv=n_kv, n_tp=n_tp, rows_block=rows_block, model_width=model_width
    )
    if aligned:
        outs = call(
            down,
            [shape_of((rows, piece_cols), F32)] + [shape_of((rows, piece_cols), BF16)] * (n_tp - 1),
            *hidden_all,
            w_down_near,
            *squares_all,
            scratch=[pltpu.VMEM((rows, block_cols), F32)],
            name="down",
        )
        mixed_own, down_own, down_send = mixed, outs[0], list(outs[1:])
    else:
        part = call(
            down,
            shape_of((rows, block_cols), F32),
            *hidden_all,
            w_down_near,
            *squares_all,
            name="down",
        )
        mixed_own, down_own = piece(mixed, 0), piece(part, 0)
        down_send = [piece(part, m).astype(BF16) for m in range(1, n_tp)]
    result = call(
        functools.partial(last_kernel, n_kv=n_kv, rows_block=rows_block),
        shape_of((rows, piece_cols), BF16),
        mixed_own,
        down_own,
        *exchange([None] + down_send, "tp"),
        name="last",
    )
    return (result, new_state)


def solution(mesh):
    in_specs = (
        P("grp", ("kv", "tp")),
        P(("grp", "kv")),
        P(("grp", "kv"), "tp", None, None),
        P(("grp", "kv"), None, "tp"),
        P(("grp", "kv"), None, "tp"),
        P(("grp", "kv"), None, "tp"),
        P(),
        P("kv", "tp"),
        P("kv", "tp"),
        P("kv", "tp"),
        P("kv", "tp"),
        P(),
        P(),
        P(),
        P(),
        P(),
        P(),
        P(),
        P(),
        P("tp", "kv"),
        P(),
        P("kv", "tp"),
        P("tp", "kv"),
    )
    out_specs = (P("grp", ("kv", "tp")), P(("grp", "kv"), "tp", None, None))
    return jax.shard_map(
        on_device, mesh=mesh, in_specs=in_specs, out_specs=out_specs, check_vma=False
    )
```

```python
import functools

import jax
import jax.numpy as jnp
from jax import lax
from jax.experimental import pallas as pl
from jax.experimental.pallas import tpu as pltpu
from jax.sharding import PartitionSpec as P

EPSILON = 1e-06
LANES = 128
MIB = 1024 * 1024
F32 = jnp.float32
BF16 = jnp.bfloat16


def shape_of(shape, dtype):
    return jax.ShapeDtypeStruct(shape, dtype)


def call(body, outs, *args, scratch=(), name):
    return pl.pallas_call(
        body,
        out_shape=outs,
        scratch_shapes=list(scratch),
        name=name,
        compiler_params=pltpu.CompilerParams(vmem_limit_bytes=16 * MIB),
    )(*args)


def send(values, axis, distance):
    size = lax.axis_size(axis)
    return lax.ppermute(values, axis, [(i, i ^ distance) for i in range(size)])


def exchange(blocks, axis, order=None):
    got = {m: send(blocks[m], axis, m) for m in order or reversed(range(1, len(blocks)))}
    return [got[m] for m in order or range(1, len(blocks))]


def silu(values):
    return values * jax.nn.sigmoid(values)


def fetch_kernel(*refs, count):
    sources, targets, sems = refs[:count], refs[count : 2 * count], refs[2 * count]
    copies = []
    for index in range(count):
        source, target = sources[index], targets[index]
        if source.shape != target.shape:
            first = pl.multiple_of(lax.axis_index("kv") * target.shape[1], target.shape[1])
            source = source.at[:, pl.ds(first, target.shape[1])]
        copies.append(pltpu.make_async_copy(source, target, sems.at[index]))
    for copy in copies:
        copy.start()
    for copy in copies:
        copy.wait()


def fetch(*arrays, name, columns=None):
    shapes = [array.shape for array in arrays]
    if columns:
        shapes = [(shape[0], count) for shape, count in zip(shapes, columns)]
    return pl.pallas_call(
        functools.partial(fetch_kernel, count=len(arrays)),
        in_specs=[pl.BlockSpec(memory_space=pltpu.HBM)] * len(arrays),
        out_specs=[pl.BlockSpec(memory_space=pltpu.VMEM)] * len(arrays),
        out_shape=[pltpu.VMEM(shape, array.dtype) for shape, array in zip(shapes, arrays)],
        scratch_shapes=[pltpu.SemaphoreType.DMA((len(arrays),))],
        name=name,
        compiler_params=pltpu.CompilerParams(vmem_limit_bytes=MIB),
    )(*[pltpu.with_memory_space_constraint(array, pltpu.HBM) for array in arrays])


def row_of(ref, index):
    values = ref[...].astype(F32)
    place = lax.broadcasted_iota(jnp.int32, values.shape, 0)
    return jnp.sum(jnp.where(place == index, values, 0.0), axis=0, keepdims=True)


def project_kernel(*refs, pieces, rows_block, n_kv, heads, block_cols):
    piece_refs = refs[:pieces]
    gain_ref, w_query_ref, w_key_ref, w_value_ref, w_beta_ref, w_decay_ref = refs[
        pieces : pieces + 6
    ]
    scaled_ref, own_ref = refs[pieces + 6 : pieces + 8]
    out_refs = refs[pieces + 8 :]
    kv_place, tp_place = lax.axis_index("kv"), lax.axis_index("tp")
    squares = [0.0] * n_kv
    for m in range(pieces):
        width = piece_refs[m].shape[1]
        first = pl.multiple_of((tp_place ^ m) * width if pieces > 1 else 0, LANES)
        gain_row = kv_place * (block_cols // LANES) + first // LANES
        gain = jnp.concatenate(
            [row_of(gain_ref, gain_row + j) for j in range(width // LANES)], axis=1
        )
        for d in range(n_kv):
            row = pl.multiple_of((kv_place ^ d) * rows_block, rows_block)
            wide = piece_refs[m][pl.ds(row, rows_block), :].astype(F32)
            squares[d] = squares[d] + jnp.sum(wide * wide, axis=1, keepdims=True)
            scaled_ref[d * rows_block : (d + 1) * rows_block, pl.ds(first, width)] = (
                wide * gain
            ).astype(BF16)
    scaled = scaled_ref[...]
    first = 0
    for w_ref in (w_query_ref, w_key_ref, w_value_ref):
        part = jnp.dot(scaled, w_ref[...], preferred_element_type=F32)
        cols = slice(first, first + w_ref.shape[1])
        first = first + w_ref.shape[1]
        own_ref[:, cols] = part[:rows_block]
        for d in range(1, n_kv):
            out_refs[d - 1][:, cols] = part[d * rows_block : (d + 1) * rows_block].astype(BF16)
    lane = lax.broadcasted_iota(jnp.int32, (scaled.shape[0], LANES), 1)
    total_heads = w_beta_ref.shape[0]

    def small_dot(w_ref, place):
        part = lax.dot_general(
            scaled, w_ref[...], (((1,), (1,)), ((), ())), preferred_element_type=F32
        )
        part = jnp.pad(part, ((0, 0), (0, LANES - total_heads)))
        return pltpu.roll(part, LANES + place - tp_place * heads, 1)

    small = jnp.where(lane < heads, small_dot(w_beta_ref, 0), small_dot(w_decay_ref, heads))
    lane = lane[:rows_block]
    half = LANES // 2
    for d in range(n_kv):
        block = small[d * rows_block : (d + 1) * rows_block]
        block = jnp.where(lane == half - 1, squares[d], block)
        if d == 0:
            own_ref[:, first:] = block
        else:
            high = block.astype(BF16)
            low = (block - high.astype(F32)).astype(BF16)
            out_refs[d - 1][:, first:] = jnp.where(
                lane < half, high.astype(F32), pltpu.roll(low.astype(F32), half, 1)
            ).astype(BF16)


def gate_project_kernel(scaled_ref, w_ref, after_ref, own_ref, *out_refs, rows_block):
    del after_ref
    part = jnp.dot(scaled_ref[...], w_ref[...], preferred_element_type=F32)
    own_ref[...] = part[:rows_block]
    for d, out_ref in enumerate(out_refs, 1):
        out_ref[...] = part[d * rows_block : (d + 1) * rows_block].astype(BF16)


def store_kernel(source, weight, after_ref, target, near_ref, done_ref, sems, *, chunks):
    done_ref[...] = after_ref[...]
    size = source.shape[0] // chunks
    copies = [
        pltpu.make_async_copy(
            source.at[pl.ds(i * size, size)], target.at[pl.ds(i * size, size)], sems.at[i]
        )
        for i in range(chunks)
    ]
    copies.append(pltpu.make_async_copy(weight, near_ref, sems.at[chunks]))
    for copy in copies:
        copy.start()
    for copy in copies:
        copy.wait()


def history_kernel(lengths_ref, *refs):
    tp_place = lax.axis_index("tp")
    past, rows, _ = refs[0].shape
    row = lax.broadcasted_iota(jnp.int32, (rows, LANES), 0)
    lengths = jnp.zeros((rows, LANES), jnp.int32)
    for s in range(rows):
        lengths = jnp.where(row == s, lengths_ref[s], lengths)
    refs[9][...] = (lengths == 1).astype(F32)
    for hist_ref, taps_ref, out_ref in zip(refs[:3], refs[3:6], refs[6:9]):
        width = hist_ref.shape[2]
        taps = taps_ref[:, pl.ds(pl.multiple_of(tp_place * width, LANES), width)].astype(F32)
        total = 0.0
        for r in range(past):
            live = lengths[:, 0:1] >= past + 1 - r
            total = total + jnp.where(live, hist_ref[r].astype(F32), 0.0) * taps[r : r + 1]
        out_ref[...] = total


def delta_kernel(*refs, n_kv, heads, key_heads, head_size, model_width, step_rows):
    got_refs, refs = refs[1:n_kv], (refs[0],) + refs[n_kv:]
    own_ref, hist_q, hist_k, hist_v, fresh_ref, taps_q, taps_k, taps_v = refs[:8]
    decay_ref, bias_ref, state_ref, new_ref, readout_ref, scale_ref = refs[8:14]
    q_scr, k_scr, v_scr, dot_scr, fade_scr, strength_scr = refs[14:]
    key_cols = key_heads * head_size
    value_cols = heads * head_size
    repeat = heads // key_heads
    half = LANES // 2
    steps = q_scr.shape[1]
    tp_place = lax.axis_index("tp")

    def fold(values):
        return values.reshape(steps, step_rows, values.shape[-1])

    @pl.when(pl.program_id(0) == 0)
    def _():
        small_first = 2 * key_cols + value_cols
        small = own_ref[:, small_first:]
        for ref in got_refs:
            got = ref[:, small_first:].astype(F32)
            small = small + got + pltpu.roll(got, half, 1)
        row_scale = lax.rsqrt(small[:, half - 1 : half] / model_width + EPSILON)
        scale_ref[...] = jnp.broadcast_to(row_scale, scale_ref.shape)
        small = small * row_scale
        strength = jax.nn.sigmoid(small)
        to_decay = LANES + heads - tp_place * heads

        def by_head(ref):
            row = jnp.pad(ref[...], ((0, 7), (0, LANES - ref.shape[1])))
            return pltpu.roll(row, to_decay, 1)[0:1]

        logits = small + by_head(bias_ref)
        fade = jnp.exp(-jnp.exp(by_head(decay_ref)) * jax.nn.softplus(logits))
        fade = jnp.where(fresh_ref[...] > 0, 0.0, fade)

        def filtered(first, hist, taps_ref, head):
            cols = slice(first, first + head_size)
            total = own_ref[:, cols]
            for ref in got_refs:
                total = total + ref[:, cols].astype(F32)
            width = hist.shape[1]
            tap_first = pl.multiple_of(tp_place * width + head * head_size, LANES)
            taps = taps_ref[:, pl.ds(tap_first, head_size)].astype(F32)[-1:]
            past = hist[:, head * head_size : (head + 1) * head_size]
            return silu(total * row_scale * taps + past)

        for g in range(key_heads):
            q = filtered(g * head_size, hist_q, taps_q, g)
            q = q * lax.rsqrt(jnp.sum(q * q, axis=1, keepdims=True) + EPSILON)
            q = q * head_size ** (-0.5)
            k = filtered(key_cols + g * head_size, hist_k, taps_k, g)
            k = k * lax.rsqrt(jnp.sum(k * k, axis=1, keepdims=True) + EPSILON)
            q_scr[g] = fold(q)
            k_scr[g] = fold(k)
            dot_scr[g] = fold(jnp.broadcast_to(jnp.sum(q * k, axis=1, keepdims=True), q.shape))
        for h in range(heads):
            v = filtered(2 * key_cols + h * head_size, hist_v, taps_v, h)
            v_scr[h] = fold(v)
            fade_scr[h] = fold(jnp.broadcast_to(fade[:, heads + h : heads + h + 1], v.shape))
            strength_scr[h] = fold(jnp.broadcast_to(strength[:, h : h + 1], v.shape))

    step = pl.program_id(0)
    pair = repeat * head_size
    place = lax.broadcasted_iota(jnp.int32, (step_rows, pair), 0)
    def group(g):
        return range(g * repeat, (g + 1) * repeat)

    def wide(scr, g):
        return jnp.concatenate([scr[h, step] for h in group(g)], axis=1)

    def find(g, a, found):
        asked = jnp.concatenate([k_scr[g, step], q_scr[g, step]], axis=0).astype(BF16)
        row = step * step_rows + a
        state = jnp.concatenate([state_ref[row, h].astype(BF16) for h in group(g)], axis=1)
        now = jnp.dot(asked, state, preferred_element_type=F32)
        here = place == a
        return (
            found[0] + jnp.where(here, now[:step_rows], 0.0),
            found[1] + jnp.where(here, now[step_rows:], 0.0),
        )

    found = (0.0, 0.0)
    for a in range(step_rows):
        found = find(0, a, found)
    for g in range(key_heads):
        recalled, read = found
        found = (0.0, 0.0)
        k = k_scr[g, step]
        fade = wide(fade_scr, g)
        update = wide(strength_scr, g) * (wide(v_scr, g) - fade * recalled)
        dots = jnp.concatenate([dot_scr[g, step]] * repeat, axis=1)
        readout_ref[:, g * pair : (g + 1) * pair] = fade * read + dots * update
        if g + 1 < key_heads:
            for a in range(step_rows):
                found = find(g + 1, a, found)
        k_columns = k.T
        for a in range(step_rows):
            row = step * step_rows + a
            k_wide = jnp.broadcast_to(k_columns[:, a : a + 1], (head_size, head_size))
            for r, h in enumerate(group(g)):
                fade_row = fade_scr[h, step, a : a + 1, :]
                update_row = update[a : a + 1, r * head_size : (r + 1) * head_size]
                new_ref[row, h] = state_ref[row, h] * fade_row + k_wide * update_row


def gate_kernel(readout_ref, scale_ref, own_ref, *refs, n_kv, heads, head_size):
    got_refs, gain_ref, out_ref = refs[: n_kv - 1], refs[n_kv - 1], refs[n_kv]
    row_scale = scale_ref[:, 0:1]
    for h in range(heads):
        cols = slice(h * head_size, (h + 1) * head_size)
        gate_in = own_ref[:, cols]
        for ref in got_refs:
            gate_in = gate_in + ref[:, cols].astype(F32)
        gate_in = gate_in * row_scale
        read = readout_ref[:, cols]
        mean = jnp.sum(read * read, axis=1, keepdims=True) / head_size
        normed = read * lax.rsqrt(mean + EPSILON)
        out_ref[:, cols] = (normed * gain_ref[...].astype(F32) * silu(gate_in)).astype(BF16)


def mixer_kernel(*refs, n_kv):
    w_ref, part_ref, send_refs = refs[n_kv], refs[n_kv + 1], refs[n_kv + 2 :]
    gated = jnp.concatenate([ref[...] for ref in refs[:n_kv]], axis=0)
    part = jnp.dot(gated, w_ref[...], preferred_element_type=F32)
    part_ref[...] = part
    width = send_refs[0].shape[1]
    for index, ref in enumerate(send_refs):
        ref[...] = part[:, index * width : (index + 1) * width].astype(BF16)


def pair_kernel(part_ref, got_ref, *refs, first):
    out_ref = refs[-1]
    width = got_ref.shape[1]
    total = part_ref[:, first : first + width] + got_ref[...].astype(F32)
    out_ref[...] = total.astype(BF16)


def up_kernel(*refs, pieces, got, rows_block, n_kv, block_cols):
    piece_refs = refs[:pieces]
    part_ref, got_refs = refs[pieces], refs[pieces + 1 : pieces + 1 + got]
    gain_ref, w_ref = refs[pieces + 1 + got : pieces + 3 + got]
    mixed_ref, squares_ref, own_ref = refs[pieces + 3 + got : pieces + 6 + got]
    out_refs = refs[pieces + 6 + got : pieces + 5 + got + n_kv]
    stream_ref = refs[pieces + 5 + got + n_kv]
    kv_place, tp_place = lax.axis_index("kv"), lax.axis_index("tp")
    for m in range(pieces):
        width = piece_refs[m].shape[1]
        first = pl.multiple_of((tp_place ^ m) * width if pieces > 1 else 0, LANES)
        for d in range(n_kv):
            row = pl.multiple_of((kv_place ^ d) * rows_block, rows_block)
            stream_ref[d * rows_block : (d + 1) * rows_block, pl.ds(first, width)] = piece_refs[m][
                pl.ds(row, rows_block), :
            ].astype(F32)
    groups = block_cols // got_refs[0].shape[1]
    got_totals = []
    for index in range(groups):
        total = 0.0
        for ref in got_refs[index::groups]:
            total = total + ref[...].astype(F32)
        got_totals.append(total)
    total = part_ref[...] + jnp.concatenate(got_totals, axis=1)
    mixed = (stream_ref[...] + total).astype(BF16)
    wide = mixed.astype(F32)
    stream_ref[...] = wide
    if mixed_ref.shape[1] == block_cols:
        mixed_ref[...] = mixed
    else:
        width = mixed_ref.shape[1]
        mixed_ref[...] = stream_ref[:, pl.ds(pl.multiple_of(tp_place * width, LANES), width)].astype(
            BF16
        )
    squares = jnp.sum(wide * wide, axis=1, keepdims=True)
    squares_ref[...] = jnp.broadcast_to(squares, (squares.shape[0], LANES)).T[:8]
    gain = gain_ref[0:1, pl.ds(pl.multiple_of(kv_place * block_cols, LANES), block_cols)]
    scaled = (wide * gain.astype(F32)).astype(BF16)
    part = jnp.dot(scaled, w_ref[...], preferred_element_type=F32)
    own_ref[...] = part[:rows_block]
    for d in range(1, n_kv):
        out_refs[d - 1][...] = part[d * rows_block : (d + 1) * rows_block].astype(BF16)


def hidden_kernel(*refs):
    squares_ref, squares_out = refs[-3], refs[-1]
    squares_out[...] = squares_ref[...]
    total = refs[0][...]
    for ref in refs[1:-3]:
        total = total + ref[...].astype(F32)
    total = jnp.maximum(total, 0.0)
    refs[-2][...] = (total * total).astype(BF16)


def unit_factor(square_refs, rows_block, model_width):
    squares = square_refs[0][...]
    rows = squares.shape[1]
    block = lax.broadcasted_iota(jnp.int32, squares.shape, 1) // rows_block
    for m in range(1, len(square_refs)):
        got = square_refs[m][...]
        bit = 1
        while bit < len(square_refs):
            if m & bit:
                got = jnp.where(
                    (block & bit) == 0,
                    pltpu.roll(got, rows - bit * rows_block, 1),
                    pltpu.roll(got, bit * rows_block, 1),
                )
            bit *= 2
        squares = squares + got
    return (1.0 / (squares / model_width + EPSILON)).T[:, 0:1]


def down_kernel(*refs, n_kv, n_tp, rows_block, model_width):
    w_ref, own_ref = refs[n_kv], refs[2 * n_kv + 1]
    factor = unit_factor(refs[n_kv + 1 : 2 * n_kv + 1], rows_block, model_width)
    hidden = jnp.concatenate([ref[...] for ref in refs[:n_kv]], axis=0)
    part = jnp.dot(hidden, w_ref[...], preferred_element_type=F32) * factor
    if own_ref.shape == part.shape:
        own_ref[...] = part
        return
    send_refs, part_ref = refs[2 * n_kv + 2 : 2 * n_kv + 1 + n_tp], refs[2 * n_kv + 1 + n_tp]
    part_ref[...] = part
    width = own_ref.shape[1]
    for m in range(n_tp):
        first = pl.multiple_of((lax.axis_index("tp") ^ m) * width, LANES)
        piece = part_ref[:, pl.ds(first, width)]
        if m == 0:
            own_ref[...] = piece
        else:
            send_refs[m - 1][...] = piece.astype(BF16)


def last_kernel(mixed_ref, own_ref, *refs, n_kv, rows_block):
    out_ref = refs[-1]
    kv_place = lax.axis_index("kv")
    total = own_ref[...]
    for ref in refs[:-1]:
        total = total + ref[...].astype(F32)
    result = (mixed_ref[...].astype(F32) + total).astype(BF16)
    for d in range(n_kv):
        row = pl.multiple_of((kv_place ^ d) * rows_block, rows_block)
        out_ref[pl.ds(row, rows_block), :] = result[d * rows_block : (d + 1) * rows_block]


SMEM_SPEC = pl.BlockSpec(memory_space=pltpu.SMEM)
VMEM_SPEC = pl.BlockSpec(memory_space=pltpu.VMEM)


def on_device(
    stream,
    lengths,
    delta_state,
    q_hist,
    k_hist,
    v_hist,
    norm_gain,
    w_query,
    w_key,
    w_value,
    w_gate,
    w_beta,
    w_decay,
    conv_query,
    conv_key,
    conv_value,
    decay_log,
    time_bias,
    out_gain,
    w_out,
    mlp_gain,
    w_up,
    w_down,
):
    n_kv, n_tp = lax.axis_size("kv"), lax.axis_size("tp")
    model_width = norm_gain.shape[0]
    block_cols = model_width // n_kv
    piece_cols = stream.shape[1]
    aligned = piece_cols % LANES == 0
    tp_place = lax.axis_index("tp")
    rows, rows_block = stream.shape[0], delta_state.shape[0]
    heads, head_size = delta_state.shape[1], delta_state.shape[2]
    key_cols, value_cols = q_hist.shape[2], v_hist.shape[2]
    key_heads = key_cols // head_size
    count = n_kv - 1

    pieces = [stream] + exchange([stream] * n_tp, "tp")
    if not aligned:
        order = tp_place ^ jnp.arange(n_tp)
        pieces = [
            jnp.take(jnp.stack(pieces), order, axis=0).transpose(1, 0, 2).reshape(rows, block_cols)
        ]
    near = fetch(
        w_query,
        w_key,
        w_value,
        w_beta.T,
        w_decay.T,
        w_gate,
        norm_gain.reshape(model_width // LANES, LANES),
        *([stream] if aligned else []),
        name="fetch_input",
        columns=[w.shape[1] for w in (w_query, w_key, w_value)]
        + [block_cols] * 2
        + [value_cols, LANES]
        + [piece_cols] * aligned,
    )
    if aligned:
        pieces[0] = near[7]
    joined_cols = 2 * key_cols + value_cols + LANES
    outs = call(
        functools.partial(
            project_kernel,
            pieces=len(pieces),
            rows_block=rows_block,
            n_kv=n_kv,
            heads=heads,
            block_cols=block_cols,
        ),
        [shape_of((rows, block_cols), BF16), shape_of((rows_block, joined_cols), F32)]
        + [shape_of((rows_block, joined_cols), BF16)] * count,
        *pieces,
        near[6],
        *near[:5],
        name="project",
    )
    scaled, joined_own = outs[0], outs[1]
    order = sorted(range(1, n_kv), key=lambda m: (m != n_kv - 1, m))
    joined_got = exchange([None] + list(outs[2:]), "kv", order)
    (state,) = fetch(delta_state, name="fetch_state")
    outs = call(
        functools.partial(gate_project_kernel, rows_block=rows_block),
        [shape_of((rows_block, value_cols), F32)]
        + [shape_of((rows_block, value_cols), BF16)] * count,
        scaled,
        near[5],
        state,
        name="gate_project",
    )
    gate_own = outs[0]
    gate_got = exchange([None] + list(outs[1:]), "kv")

    hist = pl.pallas_call(
        history_kernel,
        in_specs=[SMEM_SPEC] + [VMEM_SPEC] * 6,
        out_shape=[
            shape_of((rows_block, width), F32) for width in (key_cols, key_cols, value_cols, LANES)
        ],
        name="history",
        compiler_params=pltpu.CompilerParams(vmem_limit_bytes=8 * MIB),
    )(
        lengths,
        *[array.transpose(1, 0, 2) for array in (q_hist, k_hist, v_hist)],
        conv_query,
        conv_key,
        conv_value,
    )

    step_rows = 8
    steps = rows_block // step_rows
    state_near, readout, row_scale = pl.pallas_call(
        functools.partial(
            delta_kernel,
            n_kv=n_kv,
            heads=heads,
            key_heads=key_heads,
            head_size=head_size,
            model_width=model_width,
            step_rows=step_rows,
        ),
        grid=(steps,),
        in_specs=[VMEM_SPEC] * (n_kv + 10),
        out_specs=[
            VMEM_SPEC,
            pl.BlockSpec((step_rows, value_cols), lambda i: (i, 0)),
            pl.BlockSpec((rows_block, LANES), lambda i: (0, 0)),
        ],
        out_shape=[
            pltpu.VMEM(delta_state.shape, F32),
            shape_of((rows_block, value_cols), F32),
            shape_of((rows_block, LANES), F32),
        ],
        input_output_aliases={n_kv + 9: 0},
        scratch_shapes=[
            pltpu.VMEM((key_heads, steps, step_rows, head_size), F32),
            pltpu.VMEM((key_heads, steps, step_rows, head_size), F32),
            pltpu.VMEM((heads, steps, step_rows, head_size), F32),
            pltpu.VMEM((key_heads, steps, step_rows, head_size), F32),
            pltpu.VMEM((heads, steps, step_rows, head_size), F32),
            pltpu.VMEM((heads, steps, step_rows, head_size), F32),
        ],
        name="delta",
        compiler_params=pltpu.CompilerParams(
            vmem_limit_bytes=8 * MIB, dimension_semantics=("arbitrary",)
        ),
    )(
        joined_own,
        *joined_got,
        *hist,
        conv_query,
        conv_key,
        conv_value,
        decay_log.reshape(1, -1),
        time_bias.reshape(1, -1),
        state,
    )
    gated = call(
        functools.partial(gate_kernel, n_kv=n_kv, heads=heads, head_size=head_size),
        shape_of((rows_block, value_cols), BF16),
        readout,
        row_scale,
        gate_own,
        *gate_got,
        out_gain.reshape(1, head_size),
        name="gate",
    )
    gated_all = [gated] + exchange([gated] * n_kv, "kv")
    halves = 2 if n_tp == 4 and block_cols % (2 * LANES) == 0 else 1
    half_block = shape_of((rows, block_cols // halves), BF16)
    outs = call(
        functools.partial(mixer_kernel, n_kv=n_kv),
        [shape_of((rows, block_cols), F32)] + [half_block] * halves,
        *gated_all,
        w_out,
        name="mixer",
    )
    mixer_part, mixer_send = outs[0], list(outs[1:])
    if halves == 2:
        mixer_got, before = [None] * 4, []
        for index, (near_step, far_step) in enumerate(((1, 2), (2, 1))):
            mixer_got[index] = send(mixer_send[index], "tp", near_step)
            pair = call(
                functools.partial(pair_kernel, first=index * block_cols // 2),
                half_block,
                mixer_part,
                mixer_got[index],
                *before,
                name=f"pair_{index}",
            )
            before = [pair]
            mixer_got[2 + index] = send(pair, "tp", far_step)
    else:
        mixer_got = exchange(mixer_send * n_tp, "tp")
    unit_cols = w_up.shape[1]
    outs = call(
        functools.partial(
            up_kernel,
            pieces=len(pieces),
            got=len(mixer_got),
            rows_block=rows_block,
            n_kv=n_kv,
            block_cols=block_cols,
        ),
        [
            shape_of((rows, piece_cols if aligned else block_cols), BF16),
            shape_of((8, rows), F32),
            shape_of((rows_block, unit_cols), F32),
        ]
        + [shape_of((rows_block, unit_cols), BF16)] * count,
        *pieces,
        mixer_part,
        *mixer_got,
        mlp_gain.reshape(1, model_width),
        w_up,
        scratch=[pltpu.VMEM((rows, block_cols), F32)],
        name="up",
    )
    mixed, squares, up_own = outs[0], outs[1], outs[2]
    chunks = 4
    new_state, w_down_near, squares = pl.pallas_call(
        functools.partial(store_kernel, chunks=chunks),
        in_specs=[VMEM_SPEC, pl.BlockSpec(memory_space=pltpu.HBM), VMEM_SPEC],
        out_specs=[pl.BlockSpec(memory_space=pltpu.HBM), VMEM_SPEC, VMEM_SPEC],
        out_shape=[
            shape_of(delta_state.shape, F32),
            pltpu.VMEM(w_down.shape, BF16),
            shape_of(squares.shape, F32),
        ],
        scratch_shapes=[pltpu.SemaphoreType.DMA((chunks + 1,))],
        name="store_state",
        compiler_params=pltpu.CompilerParams(vmem_limit_bytes=MIB),
    )(state_near, pltpu.with_memory_space_constraint(w_down, pltpu.HBM), squares)
    hidden, squares = call(
        hidden_kernel,
        [shape_of((rows_block, unit_cols), BF16), shape_of((8, rows), F32)],
        up_own,
        *exchange([None] + list(outs[3:]), "kv", order),
        squares,
        name="hidden",
    )
    hidden_all = [hidden] + exchange([hidden] * n_kv, "kv")
    squares_all = [squares] + exchange([squares] * n_kv, "kv")

    def piece(array, distance):
        return lax.dynamic_slice_in_dim(array, (tp_place ^ distance) * piece_cols, piece_cols, 1)

    down = functools.partial(
        down_kernel, n_kv=n_kv, n_tp=n_tp, rows_block=rows_block, model_width=model_width
    )
    if aligned:
        outs = call(
            down,
            [shape_of((rows, piece_cols), F32)] + [shape_of((rows, piece_cols), BF16)] * (n_tp - 1),
            *hidden_all,
            w_down_near,
            *squares_all,
            scratch=[pltpu.VMEM((rows, block_cols), F32)],
            name="down",
        )
        mixed_own, down_own, down_send = mixed, outs[0], list(outs[1:])
    else:
        part = call(
            down,
            shape_of((rows, block_cols), F32),
            *hidden_all,
            w_down_near,
            *squares_all,
            name="down",
        )
        mixed_own, down_own = piece(mixed, 0), piece(part, 0)
        down_send = [piece(part, m).astype(BF16) for m in range(1, n_tp)]
    result = call(
        functools.partial(last_kernel, n_kv=n_kv, rows_block=rows_block),
        shape_of((rows, piece_cols), BF16),
        mixed_own,
        down_own,
        *exchange([None] + down_send, "tp", [*range(2, n_tp), 1]),
        name="last",
    )
    return (result, new_state)


def solution(mesh):
    in_specs = (
        P("grp", ("kv", "tp")),
        P(("grp", "kv")),
        P(("grp", "kv"), "tp", None, None),
        P(("grp", "kv"), None, "tp"),
        P(("grp", "kv"), None, "tp"),
        P(("grp", "kv"), None, "tp"),
        P(),
        P("kv", "tp"),
        P("kv", "tp"),
        P("kv", "tp"),
        P("kv", "tp"),
        P(),
        P(),
        P(),
        P(),
        P(),
        P(),
        P(),
        P(),
        P("tp", "kv"),
        P(),
        P("kv", "tp"),
        P("tp", "kv"),
    )
    out_specs = (P("grp", ("kv", "tp")), P(("grp", "kv"), "tp", None, None))
    return jax.shard_map(
        on_device, mesh=mesh, in_specs=in_specs, out_specs=out_specs, check_vma=False
    )
```
